256 devices in a mesh: ep: 16 (over y, x), tp: 16 (over z, core).
Axes of the slice: x: 4, y: 4, z: 8, core: 2. Of those that a mesh axis runs over, the one named last changes fastest.
Arguments:
- hidden: bfloat16 [512, 2048], P('ep'), may hold values from -6 to 6
- attn_gain: float32 [2048], replicated, may hold values from 0.1 to 1.9
- query_weight: bfloat16 [2048, 1024], P(None, 'tp'), may hold values from -0.125 to 0.125
- rotary_weight: bfloat16 [2048, 512], P(None, 'tp'), may hold values from -0.125 to 0.125
- key_up: bfloat16 [16, 64, 512], P('tp'), may hold values from -0.75 to 0.75
- cache_latent: bfloat16 [512, 4096, 512], P(('ep', 'tp'))
- cache_rotary: bfloat16 [512, 32, 4096], P(('ep', 'tp')), may hold values from -6 to 6
- lengths: int32 [512], P(('ep', 'tp')), may hold values from 1 to 4096, as said below
- value_up: bfloat16 [16, 512, 64], P('tp'), may hold values from -0.25 to 0.25
- out_weight: bfloat16 [1024, 2048], P('tp'), may hold values from -0.1875 to 0.1875
- mixed_gain: float32 [2048], replicated, may hold values from 0.1 to 1.9
- moe_gain: float32 [2048], replicated, may hold values from 0.1 to 1.9
- expert_ids: int32 [512, 2], replicated, may hold values from 0 to 15, all different within a row; in each aligned block of 32 rows (0 to 31, 32 to 63, ...) at most 8 rows name the same one
- route_logits: float32 [512, 2], replicated, may hold values from -6 to 6
- gate_weight: bfloat16 [16, 2048, 7168], P('ep', None, 'tp'), may hold values from -0.125 to 0.125
- up_weight: bfloat16 [16, 2048, 7168], P('ep', None, 'tp'), may hold values from -0.125 to 0.125
- down_weight: bfloat16 [16, 7168, 2048], P('ep', 'tp'), may hold values from -0.0625 to 0.0625
- final_gain: float32 [2048], replicated, may hold values from 0.1 to 1.9
Outputs:
- layer_out: bfloat16 [512, 2048], P(('ep', 'tp'))
The draws below stay inside these ranges and needn't reach their ends.
Inputs may be any that keep to these rules, and one draw needn't show every extreme that they name: `lengths`: some sequence has exactly 4096 filled positions. `expert_ids`: within each aligned block of 32 rows no expert is named more than 8 times, a bound that some block reaches.
All inputs are finite; a program needn't handle non-finite values.
Results may differ from the reference program's by a relative error of at most 0.023.
The reference program's roundings to bfloat16 on the way count: a program that leaves them out, or rounds other values in their place, can miss the bound.
Values may be sent and summed in bfloat16 or wider, within the bound.
No kernel may reach another device: no remote copies, remote signals or barrier semaphores. Data moves between devices by JAX's collectives and lax.ppermute only.
A program may use at most 64 MiB of HBM per device.

```python
import math
import jax
import jax.numpy as jnp
import numpy as np
from jax import lax

D = 2048
HEADS = 16
NOPE = 64
ROPE = 32
VDIM = 64
LATENT = 512
EXPERT_FF = 7168
TOPK = 2
CACHE = 4096
SEQ_GROUP = 32
SEQS = 512
EXPERTS = 16
CAP = 8
N_EP = 16


def draw_cache_latent(key, part):
    normal_key = jax.random.fold_in(jax.random.fold_in(key, 11), 0)
    values = jax.random.normal(normal_key, (SEQS, CACHE, LATENT), jnp.float32)
    return values.astype(jnp.bfloat16)


def draw_lengths(key, part):
    first_key, second_key, pick_key = jax.random.split(jax.random.fold_in(key, 23), 3)
    first_draw = jax.random.randint(first_key, (SEQS,), 0, CACHE)
    second_draw = jax.random.randint(second_key, (SEQS,), 0, CACHE)
    filled = 1 + first_draw * second_draw // CACHE
    chosen_row = jax.random.randint(pick_key, (), 0, SEQS)
    return filled.at[chosen_row].set(CACHE).astype(jnp.int32)


def shard_levels(rng, dims, pieces, smallest, high):
    def one(axis_at, blocks):
        steps = jax.random.uniform(jax.random.fold_in(jax.random.fold_in(rng, 6), axis_at), (blocks,), jnp.float32, smallest / len(pieces), high / len(pieces))
        return jnp.repeat(jnp.exp(steps), dims[axis_at] // blocks).reshape((-1,) + (1,) * (len(dims) - axis_at - 1))

    gain = one(*pieces[0])
    for cut in pieces[1:]:
        gain = gain * one(*cut)
    return gain


def shared_out(stream_key, own, number, rows, count, top, most, slope):
    ranking = jax.random.permutation(stream_key, count)
    crowded, ordinary = load_shares(count, rows * top, most, slope, True), load_shares(count, rows * top, most, slope, False)
    places = jnp.arange(count)

    def named(sizes, turn):
        used = int((sizes > 0).sum())
        fixed = max(1, used // 4)
        shifted = fixed + (places - fixed + turn * (used - fixed)) % max(1, count - fixed)
        return jnp.zeros((count,), jnp.int32).at[ranking[jnp.where(places < fixed, places, shifted)]].set(jnp.asarray(sizes, jnp.int32))

    sizes = jnp.where(number % 4 == 0, named(crowded, number // 4), named(ordinary, number - number // 4 - 1))
    mixed = jax.random.permutation(jax.random.fold_in(own, 3), count)
    donor, receiver = mixed[0:count // 2 * 2:2], mixed[1:count // 2 * 2:2]
    slack = jnp.minimum(sizes[donor] - 1, most - sizes[receiver]) // 2
    slack = jnp.where((donor == ranking[0]) | (receiver == ranking[0]) | (sizes[receiver] == 0), 0, jnp.maximum(slack, 0))
    shifted = jax.random.randint(jax.random.fold_in(own, 4), (count // 2,), 0, 1 << 20) % (slack + 1)
    sizes = sizes.at[donor].add(-shifted).at[receiver].add(shifted)
    labels = jnp.searchsorted(jnp.cumsum(sizes), jnp.arange(rows * top), side="right").astype(jnp.int32)
    table = labels.reshape(top, rows).T
    table = table[jax.random.permutation(jax.random.fold_in(own, 1), rows)]
    turn = jax.random.randint(jax.random.fold_in(own, 2), (rows, 1), 0, top)
    return jnp.take_along_axis(table, (jnp.arange(top)[None, :] + turn) % top, axis=1)


def load_shares(count, total, reach, lean, full):
    portions = [(1 << 20) // math.isqrt(grade ** lean) + 1 for grade in range(1, count + 1)]
    largest = reach if full else min(reach, max(-(-total // count), total * portions[0] // sum(portions)))
    least = 1 if total - largest >= count - 1 else 0
    counts, spare = [largest] + [least] * (count - 1), total - largest - least * (count - 1)
    while spare > 0:
        free = [i for i in range(1, count) if counts[i] < largest] or [i for i in range(1, count) if counts[i] < reach]
        pool, left = sum([portions[i] for i in free]), spare
        for i in free:
            more = min(reach - counts[i], max(1, left * portions[i] // pool), spare)
            counts[i] = counts[i] + more
            spare = spare - more
    return np.array(counts)


def bell_draw(rng, shape, scale, bound, pieces=(), held_as=jnp.bfloat16):
    level = shard_levels(rng, shape, pieces, -0.22, 0.18) if pieces else 1.0
    drawn = jax.random.normal(rng, shape, jnp.float32) * scale * level
    return jnp.minimum(jnp.maximum(drawn, -bound), bound).astype(held_as)


def setup_inputs(seed: int = 0) -> dict:
    streams_of = jax.random.split(jax.random.key(seed), 19)
    hidden = bell_draw(streams_of[0], (SEQS, D), 1.0, 6.0, ((0, 16),))
    attn_gain = jnp.clip(1.0 + 0.18 * jax.random.normal(streams_of[1], (D,), jnp.float32), 0.1, 1.9)
    query_weight = bell_draw(streams_of[2], (D, HEADS * NOPE), D ** -0.5, 0.125, ((1, 16),))
    rotary_weight = bell_draw(streams_of[3], (D, HEADS * ROPE), D ** -0.5, 0.125, ((1, 16),))
    key_up = bell_draw(streams_of[4], (HEADS, NOPE, LATENT), NOPE ** -0.5, 0.75, ((0, 16),))
    cache_latent = draw_cache_latent(jax.random.fold_in(streams_of[18], 71), 0)
    cache_rotary = bell_draw(streams_of[6], (SEQS, ROPE, CACHE), 1.0, 6.0, ((0, 256),))
    lengths = draw_lengths(jax.random.fold_in(streams_of[18], 71), 0)
    value_up = bell_draw(streams_of[8], (HEADS, LATENT, VDIM), LATENT ** -0.5, 0.25, ((0, 16),))
    out_weight = bell_draw(streams_of[9], (HEADS * VDIM, D), (HEADS * VDIM) ** -0.5, 0.1875, ((0, 16),))
    mixed_gain = jnp.clip(1.0 + 0.18 * jax.random.normal(streams_of[10], (D,), jnp.float32), 0.1, 1.9)
    moe_gain = jnp.clip(1.0 + 0.18 * jax.random.normal(streams_of[11], (D,), jnp.float32), 0.1, 1.9)
    expert_ids_keys = jax.random.split(jax.random.fold_in(streams_of[12], 1), SEQS // SEQ_GROUP)
    expert_ids_turns = jax.random.permutation(jax.random.fold_in(streams_of[12], 3), SEQS // SEQ_GROUP)
    expert_ids = jax.vmap(lambda own, number: shared_out(jax.random.fold_in(streams_of[12], 2), own, number, SEQ_GROUP, EXPERTS, TOPK, CAP, 2))(expert_ids_keys, expert_ids_turns).reshape((SEQS, TOPK))
    route_logits = bell_draw(streams_of[13], (SEQS, TOPK), 1.0, 6.0, (), jnp.float32)
    gate_weight = bell_draw(streams_of[14], (EXPERTS, D, EXPERT_FF), D ** -0.5, 0.125, ((0, 16), (2, 16)))
    up_weight = bell_draw(streams_of[15], (EXPERTS, D, EXPERT_FF), D ** -0.5, 0.125, ((0, 16), (2, 16)))
    down_weight = bell_draw(streams_of[16], (EXPERTS, EXPERT_FF, D), EXPERT_FF ** -0.5, 0.0625, ((0, 16), (1, 16)))
    final_gain = jnp.clip(1.0 + 0.18 * jax.random.normal(streams_of[17], (D,), jnp.float32), 0.1, 1.9)
    return dict(hidden=hidden, attn_gain=attn_gain, query_weight=query_weight, rotary_weight=rotary_weight, key_up=key_up, cache_latent=cache_latent, cache_rotary=cache_rotary, lengths=lengths, value_up=value_up, out_weight=out_weight, mixed_gain=mixed_gain, moe_gain=moe_gain, expert_ids=expert_ids, route_logits=route_logits, gate_weight=gate_weight, up_weight=up_weight, down_weight=down_weight, final_gain=final_gain)


EPSILON = 1e-06

def norm_rows(values, gain_vector):
    values = values.astype(jnp.float32)
    factor = lax.rsqrt(lax.optimization_barrier(jnp.mean(values * values, axis=-1, keepdims=True)) + EPSILON)
    return values * factor * gain_vector

def rotate(values, position):
    half_width = values.shape[-1] // 2
    inverse = 10000.0 ** (-jnp.arange(half_width, dtype=jnp.float32) / half_width)
    angles = position.astype(jnp.float32)[:, None, None] * inverse
    cosine = jnp.cos(angles)
    sine_part = jnp.sin(angles)
    first_half = values[..., :half_width]
    second = values[..., half_width:]
    return jnp.concatenate([first_half * cosine - second * sine_part, second * cosine + first_half * sine_part], axis=-1)

def slot_tables(group_ids, group_probs, experts, capacity):
    row_count, top_count = group_ids.shape
    flat_ids = group_ids.reshape(-1)
    onehot = (flat_ids[:, None] == jnp.arange(experts, dtype=jnp.int32)[None, :]).astype(jnp.int32)
    earlier = jnp.cumsum(onehot, axis=0) - onehot
    slot_index = lax.optimization_barrier(jnp.sum(earlier * onehot, axis=1))
    target = flat_ids * capacity + slot_index
    source = jnp.arange(row_count * top_count, dtype=jnp.int32) // top_count
    slot_rows = jnp.full((experts * capacity,), row_count, jnp.int32).at[target].set(source)
    slot_gates = jnp.zeros((experts * capacity,), jnp.float32).at[target].set(group_probs.reshape(-1))
    return (slot_rows, slot_gates)

def reference(hidden, attn_gain, query_weight, rotary_weight, key_up, cache_latent, cache_rotary, lengths, value_up, out_weight, mixed_gain, moe_gain, expert_ids, route_logits, gate_weight, up_weight, down_weight, final_gain):
    normed_in = norm_rows(hidden, attn_gain).astype(jnp.bfloat16)
    query_nope = jnp.dot(normed_in, query_weight, preferred_element_type=jnp.float32).astype(jnp.bfloat16)
    query_nope = query_nope.reshape(SEQS, HEADS, NOPE)
    query_pe = jnp.dot(normed_in, rotary_weight, preferred_element_type=jnp.float32).astype(jnp.bfloat16)
    query_pe = query_pe.reshape(SEQS, HEADS, ROPE)
    query_latent = jnp.einsum('shn,hnc->shc', query_nope.astype(jnp.float32), key_up.astype(jnp.float32)).astype(jnp.bfloat16)
    query_rot = rotate(query_pe.astype(jnp.float32), lengths - 1).astype(jnp.bfloat16)
    score_scale = (NOPE + ROPE) ** (-0.5)

    def attend_one(operands):
        latent_query, rotary_query, latent, rope_keys, length = operands
        scores = jnp.dot(latent_query, latent.T, preferred_element_type=jnp.float32)
        scores = (scores + jnp.dot(rotary_query, rope_keys, preferred_element_type=jnp.float32)) * score_scale
        visible = jnp.arange(CACHE, dtype=jnp.int32)[None, :] < length
        scores = jnp.where(visible, scores, -jnp.inf)
        highest = lax.optimization_barrier(jnp.max(scores, axis=-1, keepdims=True))
        weights = jnp.exp(scores - highest)
        probs = (weights / lax.optimization_barrier(jnp.sum(weights, axis=-1, keepdims=True))).astype(jnp.bfloat16)
        return jnp.dot(probs, latent, preferred_element_type=jnp.float32).astype(jnp.bfloat16)
    out_latent = lax.map(attend_one, (query_latent, query_rot, cache_latent, cache_rotary, lengths))
    head_out = jnp.einsum('shc,hcv->shv', out_latent.astype(jnp.float32), value_up.astype(jnp.float32)).astype(jnp.bfloat16)
    attended = jnp.dot(head_out.reshape(SEQS, HEADS * VDIM), out_weight, preferred_element_type=jnp.float32).astype(jnp.bfloat16)
    mixed_rows = (hidden.astype(jnp.float32) + norm_rows(attended, mixed_gain)).astype(jnp.bfloat16)
    normed = norm_rows(mixed_rows, moe_gain).astype(jnp.bfloat16)
    gate_probs = jax.nn.softmax(route_logits.astype(jnp.float32), axis=-1)

    def tables_for(group_ids, group_probs):
        return slot_tables(group_ids, group_probs, EXPERTS, CAP)
    slot_rows, slot_gates = jax.vmap(tables_for)(expert_ids.reshape(N_EP, SEQ_GROUP, TOPK), gate_probs.reshape(N_EP, SEQ_GROUP, TOPK))
    offsets = jnp.arange(N_EP, dtype=jnp.int32)[:, None] * SEQ_GROUP
    global_rows = jnp.where(slot_rows < SEQ_GROUP, slot_rows + offsets, SEQS)
    global_rows = global_rows.reshape(N_EP, EXPERTS, CAP).transpose(1, 0, 2).reshape(EXPERTS, N_EP * CAP)
    expert_gates = slot_gates.reshape(N_EP, EXPERTS, CAP).transpose(1, 0, 2).reshape(EXPERTS, N_EP * CAP)
    padded = jnp.concatenate([normed, jnp.zeros((1, D), jnp.bfloat16)], axis=0)

    def one_expert(operands):
        row_index, gate_matrix, up_matrix, down_matrix = operands
        picked = padded[row_index]
        gate_part = jnp.dot(picked, gate_matrix, preferred_element_type=jnp.float32)
        up_part = jnp.dot(picked, up_matrix, preferred_element_type=jnp.float32)
        act = (jax.nn.silu(gate_part) * up_part).astype(jnp.bfloat16)
        return jnp.dot(act, down_matrix, preferred_element_type=jnp.float32)
    expert_out = lax.map(one_expert, (global_rows, gate_weight, up_weight, down_weight))
    weighted = expert_out.reshape(EXPERTS * N_EP * CAP, D) * expert_gates.reshape(-1)[:, None]
    combined = jnp.zeros((SEQS + 1, D), jnp.float32).at[global_rows.reshape(-1)].add(weighted)
    routed = combined[:SEQS].astype(jnp.bfloat16)
    return (mixed_rows.astype(jnp.float32) + norm_rows(routed, final_gain)).astype(jnp.bfloat16)
```

```python
import functools

import jax
import jax.numpy as jnp
from jax import lax
from jax.experimental import pallas as pl
from jax.experimental.pallas import tpu as pltpu
from jax.sharding import PartitionSpec as P

EPSILON = 1e-06
BLOCK = 1024
NEG = float("-inf")
VMEM = pl.BlockSpec(memory_space=pltpu.VMEM)
SMEM = pl.BlockSpec(memory_space=pltpu.SMEM)
ANY = pl.BlockSpec(memory_space=pl.ANY)
FULL_LIMIT = 60 * 1024 * 1024
SMALL_LIMIT = 8 * 1024 * 1024
NT = (((1,), (1,)), ((), ()))


def call(kernel, name, outs, ins, args, scratch=(), limit=SMALL_LIMIT, flops=0):
    return pl.pallas_call(
        kernel,
        out_shape=outs,
        in_specs=ins,
        out_specs=jax.tree.map(lambda _: VMEM, outs),
        scratch_shapes=list(scratch),
        compiler_params=pltpu.CompilerParams(vmem_limit_bytes=limit),
        cost_estimate=pl.CostEstimate(flops=flops, bytes_accessed=0, transcendentals=0),
        name=name,
    )(*args)


def shape(dims, dtype):
    return jax.ShapeDtypeStruct(dims, dtype)


def norm_rows(values, gain_vector):
    values = values.astype(jnp.float32)
    factor = lax.rsqrt(jnp.mean(values * values, axis=-1, keepdims=True) + EPSILON)
    return values * factor * gain_vector


def rotate(values, position):
    half_width = values.shape[-1] // 2
    inverse = 10000.0 ** (-jnp.arange(half_width, dtype=jnp.float32) / half_width)
    angles = position.astype(jnp.float32)[:, None, None] * inverse
    cosine = jnp.cos(angles)
    sine_part = jnp.sin(angles)
    first_half = values[..., :half_width]
    second = values[..., half_width:]
    return jnp.concatenate(
        [first_half * cosine - second * sine_part, second * cosine + first_half * sine_part],
        axis=-1,
    )


def query_kernel(hidden_ref, gain_ref, query_ref, rotary_ref, key_ref, out_ref):
    latent = key_ref.shape[1]
    normed = norm_rows(hidden_ref[...], gain_ref[...]).astype(jnp.bfloat16)
    nope = lax.dot_general(
        normed, query_ref[...], NT, preferred_element_type=jnp.float32
    ).astype(jnp.bfloat16)
    turned = lax.dot_general(normed, rotary_ref[...], NT, preferred_element_type=jnp.float32)
    out_ref[:, :latent] = jnp.dot(
        nope, key_ref[...], preferred_element_type=jnp.float32
    ).astype(jnp.bfloat16)
    out_ref[:, latent:] = turned.astype(jnp.bfloat16)


def queries(hidden, gain, query_weight, rotary_weight, key_up):
    rows = hidden.shape[0]
    width = key_up.shape[1] + rotary_weight.shape[1]
    return call(
        query_kernel,
        "queries",
        shape((rows, width), jnp.bfloat16),
        [VMEM] * 5,
        (hidden, gain[None, :], query_weight.T, rotary_weight.T, key_up),
    )


def attend_kernel(
    scale, lengths_ref, query_ref, rot_ref, latent_hbm, rotary_hbm, out_ref,
    latent_ref, rotary_ref, s_ref, latent_sems, rotary_sems,
):
    rows, heads, width = query_ref.shape
    most = latent_hbm.shape[1] // BLOCK

    def copies(s, b):
        at = pl.ds(b * BLOCK, BLOCK)
        return (
            pltpu.make_async_copy(
                latent_hbm.at[s, at, :], latent_ref.at[s, at, :], latent_sems.at[s, b]
            ),
            pltpu.make_async_copy(
                rotary_hbm.at[s, :, at], rotary_ref.at[s, :, at], rotary_sems.at[s, b]
            ),
        )

    counts = [lax.div(lengths_ref[s] + (BLOCK - 1), BLOCK) for s in range(rows)]
    for s in range(rows):
        for b in range(most):

            @pl.when(b < counts[s])
            def _start(s=s, b=b):
                for copy in copies(s, b):
                    copy.start()

    for s in range(rows):
        length = lengths_ref[s]
        blocks = counts[s]
        latent_query = query_ref[s]
        rotary_query = rot_ref[s]

        def score_block(b, highest):
            at = pl.multiple_of(b * BLOCK, BLOCK)
            for copy in copies(s, b):
                copy.wait()
            part = lax.dot_general(
                latent_query, latent_ref[s, pl.ds(at, BLOCK), :], NT,
                preferred_element_type=jnp.float32,
            )
            part = part + jnp.dot(
                rotary_query, rotary_ref[s, :, pl.ds(at, BLOCK)], preferred_element_type=jnp.float32
            )
            places = at + lax.broadcasted_iota(jnp.int32, (heads, BLOCK), 1)
            part = jnp.where(places < length, part * scale, NEG)
            s_ref[:, pl.ds(at, BLOCK)] = part
            return jnp.maximum(highest, jnp.max(part, axis=1, keepdims=True))

        highest = lax.fori_loop(0, blocks, score_block, jnp.full((heads, 1), NEG, jnp.float32))

        def weigh_block(b, total):
            at = pl.multiple_of(b * BLOCK, BLOCK)
            weights = jnp.exp(s_ref[:, pl.ds(at, BLOCK)] - highest)
            s_ref[:, pl.ds(at, BLOCK)] = weights
            return total + jnp.sum(weights, axis=1, keepdims=True)

        total = lax.fori_loop(0, blocks, weigh_block, jnp.zeros((heads, 1), jnp.float32))

        def sum_block(b, summed):
            at = pl.multiple_of(b * BLOCK, BLOCK)
            probs = (s_ref[:, pl.ds(at, BLOCK)] / total).astype(jnp.bfloat16)
            return summed + jnp.dot(
                probs, latent_ref[s, pl.ds(at, BLOCK), :], preferred_element_type=jnp.float32
            )

        summed = lax.fori_loop(0, blocks, sum_block, jnp.zeros((heads, width), jnp.float32))
        out_ref[s] = summed.astype(jnp.bfloat16)


def attend(query, rot, latent, rotary, lengths, scale):
    rows, heads, width = query.shape
    blocks = latent.shape[1] // BLOCK
    return call(
        functools.partial(attend_kernel, scale),
        "attend",
        shape((rows, heads, width), jnp.bfloat16),
        [SMEM, VMEM, VMEM, ANY, ANY],
        (lengths, query, rot, latent, rotary),
        scratch=(
            pltpu.VMEM(latent.shape, latent.dtype),
            pltpu.VMEM(rotary.shape, rotary.dtype),
            pltpu.VMEM((heads, latent.shape[1]), jnp.float32),
            pltpu.SemaphoreType.DMA((rows, blocks)),
            pltpu.SemaphoreType.DMA((rows, blocks)),
        ),
        limit=FULL_LIMIT,
        flops=4 * latent.size * heads,
    )


def mix_kernel(terms_ref, own_ref, mixed_gain_ref, moe_gain_ref, mixed_ref, send_ref):
    peers, rows, half = send_ref.shape
    attended = terms_ref[0].astype(jnp.float32)
    for t in range(1, peers):
        attended = attended + terms_ref[t].astype(jnp.float32)
    attended = attended.astype(jnp.bfloat16)
    mixed = (
        own_ref[...].astype(jnp.float32) + norm_rows(attended, mixed_gain_ref[...])
    ).astype(jnp.bfloat16)
    mixed_ref[...] = mixed
    normed = norm_rows(mixed, moe_gain_ref[...]).astype(jnp.bfloat16)
    for t in range(peers):
        send_ref[t] = normed[:, (t % 2) * half : (t % 2 + 1) * half]


def mix(terms, own, mixed_gain, moe_gain):
    peers, rows, features = terms.shape
    return call(
        mix_kernel,
        "mix",
        (
            shape((rows, features), jnp.bfloat16),
            shape((peers, rows, features // 2), jnp.bfloat16),
        ),
        [VMEM] * 4,
        (terms, own, mixed_gain[None, :], moe_gain[None, :]),
    )


def dispatch_kernel(target_ref, rows_ref, out_ref):
    slots, rows = out_ref.shape[0], rows_ref.shape[0]
    place = lax.broadcasted_iota(jnp.int32, (slots, rows), 0)
    taken = (place == target_ref[0:1, :]) | (place == target_ref[1:2, :])
    pick = jnp.where(taken, 1.0, 0.0).astype(jnp.bfloat16)
    out_ref[...] = jnp.dot(pick, rows_ref[...], preferred_element_type=jnp.float32).astype(
        jnp.bfloat16
    )


def dispatch(target, rows, slots):
    return call(
        dispatch_kernel,
        "dispatch",
        shape((slots, rows.shape[1]), jnp.bfloat16),
        [VMEM] * 2,
        (target, rows),
    )


def combine_kernel(target_ref, gates_ref, returned_ref, out_ref):
    rows, slots = out_ref.shape[0], returned_ref.shape[0]
    place = lax.broadcasted_iota(jnp.int32, (rows, slots), 1)
    gates = jnp.where(place == target_ref[:, 0:1], gates_ref[:, 0:1], 0.0)
    gates = gates + jnp.where(place == target_ref[:, 1:2], gates_ref[:, 1:2], 0.0)
    returned = returned_ref[...]
    total = None
    for _ in range(3):
        part = gates.astype(jnp.bfloat16)
        term = jnp.dot(part, returned, preferred_element_type=jnp.float32)
        total = term if total is None else total + term
        gates = gates - part.astype(jnp.float32)
    out_ref[...] = total.astype(jnp.bfloat16)


def combine(target, gates, returned):
    return call(
        combine_kernel,
        "combine",
        shape((target.shape[0], returned.shape[1]), jnp.bfloat16),
        [VMEM] * 3,
        (target, gates, returned),
    )


def finish_kernel(terms_ref, mixed_ref, gain_ref, out_ref):
    peers = terms_ref.shape[0]
    halves = []
    for c in range(2):
        part = terms_ref[c].astype(jnp.float32)
        for t in range(c + 2, peers, 2):
            part = part + terms_ref[t].astype(jnp.float32)
        halves.append(part)
    routed = jnp.concatenate(halves, axis=1).astype(jnp.bfloat16)
    out_ref[...] = (
        mixed_ref[...].astype(jnp.float32) + norm_rows(routed, gain_ref[...])
    ).astype(jnp.bfloat16)


def finish(terms, mixed, gain):
    return call(
        finish_kernel,
        "finish",
        shape(mixed.shape, jnp.bfloat16),
        [VMEM] * 3,
        (terms, mixed, gain[None, :]),
    )


def enter_kernel(core_ref, rows_ref, gate_ref, up_ref, gate_out, up_out):
    half = rows_ref.shape[1]
    at = pl.ds(pl.multiple_of(core_ref[0] * half, half), half)
    rows = rows_ref[...]
    gate_out[...] = lax.dot_general(rows, gate_ref[:, at], NT, preferred_element_type=jnp.float32)
    up_out[...] = lax.dot_general(rows, up_ref[:, at], NT, preferred_element_type=jnp.float32)


def leave_kernel(core_ref, rows_ref, gate_ref, up_ref, down_ref, gate_part, up_part, act_ref, out_ref):
    half = rows_ref.shape[1]
    at = pl.ds(pl.multiple_of((1 - core_ref[0]) * half, half), half)
    rows = rows_ref[...]
    gate = gate_part[...] + lax.dot_general(
        rows, gate_ref[:, at], NT, preferred_element_type=jnp.float32
    )
    up = up_part[...] + lax.dot_general(
        rows, up_ref[:, at], NT, preferred_element_type=jnp.float32
    )
    act = (gate / (1.0 + jnp.exp(-gate)) * up).astype(jnp.bfloat16)
    act_ref[...] = act
    out_ref[...] = jnp.dot(act, down_ref[:, at], preferred_element_type=jnp.float32).astype(
        jnp.bfloat16
    )


def close_kernel(core_ref, act_ref, down_ref, out_ref):
    half = out_ref.shape[1]
    at = pl.ds(pl.multiple_of(core_ref[0] * half, half), half)
    out_ref[...] = jnp.dot(act_ref[...], down_ref[:, at], preferred_element_type=jnp.float32)


def expert_rows(rows, gate_weight, up_weight, down_weight, core, pairs):
    slots, half = rows.shape
    width = gate_weight.shape[0]
    other = lax.ppermute(rows, "tp", pairs)
    gate_part, up_part = call(
        enter_kernel,
        "enter",
        (shape((slots, width), jnp.float32), shape((slots, width), jnp.float32)),
        [SMEM] + [VMEM] * 3,
        (core, rows, gate_weight, up_weight),
        flops=4 * slots * half * width,
    )
    act, sent = call(
        leave_kernel,
        "leave",
        (shape((slots, width), jnp.bfloat16), shape((slots, half), jnp.bfloat16)),
        [SMEM] + [VMEM] * 6,
        (core, other, gate_weight, up_weight, down_weight, gate_part, up_part),
        flops=6 * slots * half * width,
    )
    arrived = lax.ppermute(sent, "tp", pairs)
    kept = call(
        close_kernel,
        "close",
        shape((slots, half), jnp.float32),
        [SMEM] + [VMEM] * 2,
        (core, act, down_weight),
        flops=2 * slots * half * width,
    )
    return (kept + arrived.astype(jnp.float32)).astype(jnp.bfloat16)


def slot_targets(group_ids, experts, capacity):
    row_count, top_count = group_ids.shape
    flat_ids = group_ids.reshape(-1)
    onehot = (flat_ids[:, None] == jnp.arange(experts, dtype=jnp.int32)[None, :]).astype(jnp.int32)
    earlier = jnp.cumsum(onehot, axis=0) - onehot
    slot_index = jnp.sum(earlier * onehot, axis=1)
    return (flat_ids * capacity + slot_index).reshape(row_count, top_count)


def exchanged(array, axis):
    return lax.all_to_all(array, axis, split_axis=0, concat_axis=0, tiled=True)


def body(
    hidden,
    attn_gain,
    query_weight,
    rotary_weight,
    key_up,
    cache_latent,
    cache_rotary,
    lengths,
    value_up,
    out_weight,
    mixed_gain,
    moe_gain,
    expert_ids,
    route_logits,
    gate_weight,
    up_weight,
    down_weight,
    final_gain,
):
    group_rows, features = hidden.shape
    _, nope_width, latent_width = key_up.shape
    rotary_width = rotary_weight.shape[1]
    own_rows = cache_latent.shape[0]
    groups = lax.axis_size("ep")
    peers = lax.axis_size("tp")
    place = lax.axis_index("tp")
    core = (place % 2).astype(jnp.int32).reshape(1)
    pairs = [(i, i ^ 1) for i in range(peers)]
    half = features // 2
    top_count = expert_ids.shape[1]
    capacity = 2 * group_rows * top_count // groups

    query = queries(hidden, attn_gain, query_weight, rotary_weight, key_up[0])
    query = exchanged(query.reshape(peers, own_rows, -1), "tp")

    gate_probs = jax.nn.softmax(route_logits, axis=-1)
    group_start = lax.axis_index("ep") * group_rows
    group_ids = lax.dynamic_slice_in_dim(expert_ids, group_start, group_rows, 0)
    group_gates = lax.dynamic_slice_in_dim(gate_probs, group_start, group_rows, 0)
    target = slot_targets(group_ids, groups, capacity)
    own_hidden = lax.dynamic_slice_in_dim(hidden, place * own_rows, own_rows, 0)

    query = query.transpose(1, 0, 2)
    query_latent = query[:, :, :latent_width]
    query_pe = query[:, :, latent_width:]
    query_rot = rotate(query_pe.astype(jnp.float32), lengths - 1).astype(jnp.bfloat16)
    score_scale = (nope_width + rotary_width) ** (-0.5)
    query_latent, query_rot, target, group_gates, own_hidden = lax.optimization_barrier(
        (query_latent, query_rot, target, group_gates, own_hidden)
    )
    out_latent = attend(query_latent, query_rot, cache_latent, cache_rotary, lengths, score_scale)
    out_latent = exchanged(out_latent.transpose(1, 0, 2), "tp")
    head_out = jnp.dot(
        out_latent.reshape(group_rows, latent_width), value_up[0], preferred_element_type=jnp.float32
    ).astype(jnp.bfloat16)
    head_terms = jnp.dot(head_out, out_weight, preferred_element_type=jnp.float32)
    head_terms = head_terms.astype(jnp.bfloat16).reshape(peers, own_rows, features)
    head_terms = exchanged(head_terms, "tp")
    mixed_rows, normed = mix(head_terms, own_hidden, mixed_gain, moe_gain)
    normed = exchanged(normed, "tp").reshape(group_rows, half)
    outgoing = dispatch(target.T, normed, groups * capacity)
    arrived = exchanged(outgoing.reshape(groups, capacity, half), "ep")
    result = expert_rows(
        arrived.reshape(groups * capacity, half),
        gate_weight[0].T,
        up_weight[0].T,
        down_weight[0],
        core,
        pairs,
    )
    returned = exchanged(result.reshape(groups, capacity, half), "ep")
    combined = combine(target, group_gates, returned.reshape(groups * capacity, half))
    terms = exchanged(combined.reshape(peers, own_rows, half), "tp")
    return finish(terms, mixed_rows, final_gain)


def solution(mesh):
    placed = (
        P("ep", None),
        P(),
        P(None, "tp"),
        P(None, "tp"),
        P("tp", None, None),
        P(("ep", "tp"), None, None),
        P(("ep", "tp"), None, None),
        P(("ep", "tp")),
        P("tp", None, None),
        P("tp", None),
        P(),
        P(),
        P(),
        P(),
        P("ep", None, "tp"),
        P("ep", None, "tp"),
        P("ep", "tp", None),
        P(),
    )
    return jax.shard_map(
        body, mesh=mesh, in_specs=placed, out_specs=P(("ep", "tp"), None), check_vma=False
    )
```

```python
import functools

import jax
import jax.numpy as jnp
import numpy as np
from jax import lax
from jax.experimental import pallas as pl
from jax.experimental.pallas import tpu as pltpu
from jax.sharding import PartitionSpec as P

EPSILON = 1e-06
BLOCK = 1024
NEG = float("-inf")
VMEM = pl.BlockSpec(memory_space=pltpu.VMEM)
SMEM = pl.BlockSpec(memory_space=pltpu.SMEM)
HBM = pl.BlockSpec(memory_space=pltpu.HBM)
ATTEND_LIMIT = 14 * 1024 * 1024
SMALL_LIMIT = 8 * 1024 * 1024
NT = (((1,), (1,)), ((), ()))


def call(kernel, name, outs, ins, args, scratch=(), limit=SMALL_LIMIT, flops=0):
    return pl.pallas_call(
        kernel,
        out_shape=outs,
        in_specs=ins,
        out_specs=jax.tree.map(lambda _: VMEM, outs),
        scratch_shapes=list(scratch),
        compiler_params=pltpu.CompilerParams(vmem_limit_bytes=limit),
        cost_estimate=pl.CostEstimate(flops=flops, bytes_accessed=0, transcendentals=0),
        name=name,
    )(*args)


def shape(dims, dtype):
    return jax.ShapeDtypeStruct(dims, dtype)


def norm_rows(values, gain_vector):
    values = values.astype(jnp.float32)
    factor = lax.rsqrt(jnp.mean(values * values, axis=-1, keepdims=True) + EPSILON)
    return values * factor * gain_vector


def column(row):
    size = row.shape[1]
    same = lax.broadcasted_iota(jnp.int32, (size, size), 0) == lax.broadcasted_iota(
        jnp.int32, (size, size), 1
    )
    return jnp.sum(jnp.where(same, row, 0.0), axis=1, keepdims=True)


def front_kernel(
    capacity, hidden_hbm, gain_hbm, query_hbm, rotary_hbm, key_hbm, ids_hbm, logits_hbm, lengths_hbm,
    out_ref, own_ref, slots_ref, columns_ref, trig_ref,
    hidden_ref, gain_ref, query_ref, rotary_ref, key_ref, ids_ref, logits_ref, lengths_ref, sems,
):
    group_rows, features = hidden_ref.shape
    peers, own_rows, _ = out_ref.shape
    latent = key_ref.shape[1]
    pairs = (
        (lengths_hbm, lengths_ref),
        (ids_hbm, ids_ref),
        (logits_hbm, logits_ref),
        (hidden_hbm, hidden_ref),
        (gain_hbm, gain_ref),
        (query_hbm, query_ref),
        (rotary_hbm, rotary_ref),
        (key_hbm, key_ref),
    )
    copies = [pltpu.make_async_copy(s, d, sems.at[i]) for i, (s, d) in enumerate(pairs)]
    for copy in copies:
        copy.start()
    group, place = lax.axis_index("ep"), lax.axis_index("tp")

    copies[1].wait()
    copies[2].wait()
    ids_all = ids_ref[...].astype(jnp.float32)
    logits_all = logits_ref[...]
    ids = jnp.zeros((2, group_rows), jnp.float32)
    logits = jnp.zeros((2, group_rows), jnp.float32)
    for g in range(ids_all.shape[1] // group_rows):
        at = slice(g * group_rows, (g + 1) * group_rows)
        ids = jnp.where(group == g, ids_all[:, at], ids)
        logits = jnp.where(group == g, logits_all[:, at], logits)
    id_rows = [ids[k : k + 1, :] for k in range(2)]
    id_columns = [column(row) for row in id_rows]
    before = lax.broadcasted_iota(jnp.int32, (group_rows, group_rows), 0) < lax.broadcasted_iota(
        jnp.int32, (group_rows, group_rows), 1
    )
    top = jnp.maximum(logits[0:1, :], logits[1:2, :])
    weights = [jnp.exp(logits[k : k + 1, :] - top) for k in range(2)]
    for k in range(2):
        hits = jnp.where(before & (id_columns[0] == id_rows[k]), 1.0, 0.0)
        hits = hits + jnp.where(before & (id_columns[1] == id_rows[k]), 1.0, 0.0)
        slot = id_rows[k] * capacity + jnp.sum(hits, axis=0, keepdims=True)
        slots_ref[k : k + 1, :] = slot
        columns_ref[:, k : k + 1] = column(slot)
        columns_ref[:, 2 + k : 3 + k] = column(weights[k] / (weights[0] + weights[1]))

    copies[0].wait()
    half = trig_ref.shape[1] // 2
    lane = lax.broadcasted_iota(jnp.int32, (1, 2 * half), 1)
    inverse = jnp.zeros((1, 2 * half), jnp.float32)
    for i in range(half):
        value = float(np.float32(10000.0 ** (-i / half)))
        inverse = jnp.where((lane == i) | (lane == i + half), value, inverse)
    for s in range(own_rows):
        angles = (lengths_ref[s] - 1).astype(jnp.float32) * inverse
        turned = jnp.sin(angles)
        trig_ref[2 * s : 2 * s + 1, :] = jnp.cos(angles)
        trig_ref[2 * s + 1 : 2 * s + 2, :] = jnp.where(lane < half, -turned, turned)

    copies[3].wait()
    copies[4].wait()
    hidden = hidden_ref[...]
    normed = norm_rows(hidden, gain_ref[...]).astype(jnp.bfloat16)
    pick_row = lax.broadcasted_iota(jnp.int32, (8, group_rows), 0) + place * own_rows
    pick = jnp.where(pick_row == lax.broadcasted_iota(jnp.int32, (8, group_rows), 1), 1.0, 0.0)
    own = jnp.dot(pick.astype(jnp.bfloat16), hidden, preferred_element_type=jnp.float32)
    own_ref[...] = own[:own_rows].astype(jnp.bfloat16)
    copies[5].wait()
    copies[6].wait()
    copies[7].wait()
    nope = lax.dot_general(
        normed, query_ref[...], NT, preferred_element_type=jnp.float32
    ).astype(jnp.bfloat16)
    turned = lax.dot_general(normed, rotary_ref[...], NT, preferred_element_type=jnp.float32)
    projected = jnp.dot(nope, key_ref[...], preferred_element_type=jnp.float32)
    for t in range(peers):
        at = slice(t * own_rows, (t + 1) * own_rows)
        out_ref[t, :, :latent] = projected[at].astype(jnp.bfloat16)
        out_ref[t, :, latent:] = turned[at].astype(jnp.bfloat16)


def in_hbm(*arrays):
    return tuple(pltpu.with_memory_space_constraint(a, pltpu.HBM) for a in arrays)


def front(hidden, gain, query_weight, rotary_weight, key_up, ids, logits, lengths, peers, capacity):
    rows, features = hidden.shape
    own_rows = rows // peers
    rope, latent = rotary_weight.shape[1], key_up.shape[1]
    arrays = in_hbm(
        hidden, gain[None, :], query_weight.T, rotary_weight.T, key_up, ids.T, logits.T, lengths
    )
    held = [pltpu.VMEM(a.shape, a.dtype) for a in arrays[:-1]]
    return call(
        functools.partial(front_kernel, capacity),
        "front",
        (
            shape((peers, own_rows, latent + rope), jnp.bfloat16),
            shape((own_rows, features), jnp.bfloat16),
            shape((2, rows), jnp.float32),
            shape((rows, 4), jnp.float32),
            shape((2 * own_rows, rope), jnp.float32),
        ),
        [HBM] * 8,
        arrays,
        scratch=held + [pltpu.SMEM(lengths.shape, lengths.dtype), pltpu.SemaphoreType.DMA((8,))],
    )


def attend_kernel(
    scale, lengths_hbm, query_ref, trig_ref, latent_hbm, rotary_hbm, out_ref,
    lengths_ref, latent_ref, rotary_ref, latent_query, rotary_query, summed_ref,
    lengths_sem, latent_sems, rotary_sems,
):
    heads, rows, _ = query_ref.shape
    width, rope = latent_query.shape[2], rotary_query.shape[2]
    most = latent_hbm.shape[1] // BLOCK

    def copies(s, b):
        at = pl.ds(b * BLOCK, BLOCK)
        return (
            pltpu.make_async_copy(
                latent_hbm.at[s, at, :], latent_ref.at[s, at, :], latent_sems.at[s, b]
            ),
            pltpu.make_async_copy(
                rotary_hbm.at[s, :, at], rotary_ref.at[s, :, at], rotary_sems.at[s, b]
            ),
        )

    fetch = pltpu.make_async_copy(lengths_hbm, lengths_ref, lengths_sem)
    fetch.start()
    for s in range(rows):
        for copy in copies(s, 0):
            copy.start()
    swap = lax.broadcasted_iota(jnp.int32, (rope, rope), 0) == lax.rem(
        lax.broadcasted_iota(jnp.int32, (rope, rope), 1) + rope // 2, rope
    )
    swap = jnp.where(swap, 1.0, 0.0).astype(jnp.bfloat16)
    query = query_ref[...].astype(jnp.float32)
    for s in range(rows):
        own = jnp.concatenate([query[h, s : s + 1, :] for h in range(heads)], axis=0)
        latent_query[s] = own[:, :width].astype(jnp.bfloat16)
        plain = own[:, width:]
        turned = jnp.dot(plain.astype(jnp.bfloat16), swap, preferred_element_type=jnp.float32)
        rotary_query[s] = (
            plain * trig_ref[2 * s : 2 * s + 1, :] + turned * trig_ref[2 * s + 1 : 2 * s + 2, :]
        ).astype(jnp.bfloat16)
    fetch.wait()
    for s in range(rows):
        blocks = lax.div(lengths_ref[s] + (BLOCK - 1), BLOCK)
        for b in range(1, most):

            @pl.when(b < blocks)
            def _start(s=s, b=b):
                for copy in copies(s, b):
                    copy.start()

    @pl.loop(0, rows)
    def _sequence(s):
        length = lengths_ref[s]
        blocks = lax.div(length + (BLOCK - 1), BLOCK)
        for count in range(1, most + 1):

            @pl.when(blocks == count)
            def _attend(count=count):
                scores = []
                for b in range(count):
                    at = slice(b * BLOCK, (b + 1) * BLOCK)
                    for copy in copies(s, b):
                        copy.wait()
                    part = lax.dot_general(
                        latent_query[s], latent_ref[s, at, :], NT,
                        preferred_element_type=jnp.float32,
                    )
                    part = part + jnp.dot(
                        rotary_query[s], rotary_ref[s, :, at], preferred_element_type=jnp.float32
                    )
                    part = part * scale
                    if b == count - 1:
                        places = b * BLOCK + lax.broadcasted_iota(jnp.int32, (heads, BLOCK), 1)
                        part = jnp.where(places < length, part, NEG)
                    scores.append(part)
                highest = scores[0]
                for part in scores[1:]:
                    highest = jnp.maximum(highest, part)
                highest = jnp.max(highest, axis=1, keepdims=True)
                weights = [jnp.exp(part - highest) for part in scores]
                total = weights[0]
                for part in weights[1:]:
                    total = total + part
                factor = 1.0 / jnp.sum(total, axis=1, keepdims=True)
                summed = None
                for b in range(count):
                    probs = (weights[b] * factor).astype(jnp.bfloat16)
                    term = jnp.dot(
                        probs, latent_ref[s, b * BLOCK : (b + 1) * BLOCK, :],
                        preferred_element_type=jnp.float32,
                    )
                    summed = term if summed is None else summed + term
                summed_ref[s] = summed

    sums = [summed_ref[s] for s in range(rows)]
    for h in range(heads):
        out_ref[h] = jnp.concatenate([part[h : h + 1, :] for part in sums], axis=0).astype(
            jnp.bfloat16
        )


def attend(query, trig, latent, rotary, lengths, scale):
    heads, rows, _ = query.shape
    width, rope = latent.shape[2], rotary.shape[1]
    blocks = latent.shape[1] // BLOCK
    lengths, latent, rotary = in_hbm(lengths, latent, rotary)
    return call(
        functools.partial(attend_kernel, scale),
        "attend",
        shape((heads, rows, width), jnp.bfloat16),
        [HBM, VMEM, VMEM, HBM, HBM],
        (lengths, query, trig, latent, rotary),
        scratch=(
            pltpu.SMEM(lengths.shape, lengths.dtype),
            pltpu.VMEM(latent.shape, latent.dtype),
            pltpu.VMEM(rotary.shape, rotary.dtype),
            pltpu.VMEM((rows, heads, width), jnp.bfloat16),
            pltpu.VMEM((rows, heads, rope), jnp.bfloat16),
            pltpu.VMEM((rows, heads, width), jnp.float32),
            pltpu.SemaphoreType.DMA,
            pltpu.SemaphoreType.DMA((rows, blocks)),
            pltpu.SemaphoreType.DMA((rows, blocks)),
        ),
        limit=ATTEND_LIMIT,
        flops=4 * latent.size * heads,
    )


def row_sums(terms, rows, keep):
    place = lax.broadcasted_iota(jnp.int32, (8, terms.shape[0]), 1)
    wanted = (lax.rem(place, rows) == lax.broadcasted_iota(jnp.int32, place.shape, 0)) & keep(place)
    ones = jnp.where(wanted, 1.0, 0.0).astype(jnp.bfloat16)
    return jnp.dot(ones, terms, preferred_element_type=jnp.float32)


def mix_kernel(terms_ref, own_ref, mixed_gain_ref, moe_gain_ref, mixed_ref, send_ref):
    peers, rows, half = send_ref.shape
    attended = row_sums(terms_ref[...], rows, lambda place: place >= 0)[:rows].astype(jnp.bfloat16)
    mixed = (
        own_ref[...].astype(jnp.float32) + norm_rows(attended, mixed_gain_ref[...])
    ).astype(jnp.bfloat16)
    mixed_ref[...] = mixed
    normed = norm_rows(mixed, moe_gain_ref[...]).astype(jnp.bfloat16)
    for t in range(peers):
        send_ref[t] = normed[:, (t % 2) * half : (t % 2 + 1) * half]


def mix(terms, own, mixed_gain, moe_gain, peers):
    rows, features = own.shape
    return call(
        mix_kernel,
        "mix",
        (
            shape((rows, features), jnp.bfloat16),
            shape((peers, rows, features // 2), jnp.bfloat16),
        ),
        [VMEM] * 4,
        (terms, own, mixed_gain[None, :], moe_gain[None, :]),
    )


def dispatch_kernel(slots_ref, rows_ref, out_ref):
    slots, rows = out_ref.shape[0], rows_ref.shape[0]
    place = lax.broadcasted_iota(jnp.int32, (slots, rows), 0).astype(jnp.float32)
    taken = (place == slots_ref[0:1, :]) | (place == slots_ref[1:2, :])
    pick = jnp.where(taken, 1.0, 0.0).astype(jnp.bfloat16)
    out_ref[...] = jnp.dot(pick, rows_ref[...], preferred_element_type=jnp.float32).astype(
        jnp.bfloat16
    )


def dispatch(own_slots, rows, slots):
    return call(
        dispatch_kernel,
        "dispatch",
        shape((slots, rows.shape[1]), jnp.bfloat16),
        [VMEM] * 2,
        (own_slots, rows),
    )


def combine_kernel(columns_ref, returned_ref, out_ref):
    rows, slots = out_ref.shape[0], returned_ref.shape[0]
    place = lax.broadcasted_iota(jnp.int32, (rows, slots), 1).astype(jnp.float32)
    gates = jnp.where(place == columns_ref[:, 0:1], columns_ref[:, 2:3], 0.0)
    gates = gates + jnp.where(place == columns_ref[:, 1:2], columns_ref[:, 3:4], 0.0)
    returned = returned_ref[...]
    total = None
    for _ in range(3):
        part = gates.astype(jnp.bfloat16)
        term = jnp.dot(part, returned, preferred_element_type=jnp.float32)
        total = term if total is None else total + term
        gates = gates - part.astype(jnp.float32)
    out_ref[...] = total.astype(jnp.bfloat16)


def combine(columns, returned):
    return call(
        combine_kernel,
        "combine",
        shape((columns.shape[0], returned.shape[1]), jnp.bfloat16),
        [VMEM] * 2,
        (columns, returned),
    )


def finish_kernel(terms_ref, mixed_ref, gain_ref, out_ref):
    rows = mixed_ref.shape[0]
    terms = terms_ref[...]
    halves = [
        row_sums(terms, rows, lambda place, c=c: lax.rem(lax.div(place, rows), 2) == c)
        for c in range(2)
    ]
    routed = jnp.concatenate(halves, axis=1)[:rows].astype(jnp.bfloat16)
    out_ref[...] = (
        mixed_ref[...].astype(jnp.float32) + norm_rows(routed, gain_ref[...])
    ).astype(jnp.bfloat16)


def finish(terms, mixed, gain):
    return call(
        finish_kernel,
        "finish",
        shape(mixed.shape, jnp.bfloat16),
        [VMEM] * 3,
        (terms, mixed, gain[None, :]),
    )


def half_at(own, half):
    core = lax.rem(lax.axis_index("tp"), 2)
    if not own:
        core = 1 - core
    return pl.ds(pl.multiple_of(core * half, half), half)


def product(rows, weight):
    return lax.dot_general(rows, weight, NT, preferred_element_type=jnp.float32)


def enter_kernel(rows_ref, gate_ref, up_hbm, gate_out, up_out, up_ref, sem):
    half = rows_ref.shape[1]
    at = half_at(True, half)
    copy = pltpu.make_async_copy(up_hbm.at[:, at], up_ref, sem)
    copy.start()
    rows = rows_ref[...]
    gate_out[...] = product(rows, gate_ref[:, at])
    copy.wait()
    up_out[...] = product(rows, up_ref[...])


def leave_kernel(
    rows_ref, gate_ref, up_hbm, down_hbm, gate_part, up_part, act_ref, out_ref, up_ref, down_ref, sems
):
    half = rows_ref.shape[1]
    at = half_at(False, half)
    copies = [
        pltpu.make_async_copy(up_hbm.at[:, at], up_ref, sems.at[0]),
        pltpu.make_async_copy(down_hbm.at[:, at], down_ref, sems.at[1]),
    ]
    for copy in copies:
        copy.start()
    rows = rows_ref[...]
    gate = gate_part[...] + product(rows, gate_ref[:, at])
    copies[0].wait()
    up = up_part[...] + product(rows, up_ref[...])
    act = (gate / (1.0 + jnp.exp(-gate)) * up).astype(jnp.bfloat16)
    act_ref[...] = act
    copies[1].wait()
    out_ref[...] = jnp.dot(act, down_ref[...], preferred_element_type=jnp.float32).astype(
        jnp.bfloat16
    )


def close_kernel(act_ref, down_hbm, out_ref, down_ref, sem):
    copy = pltpu.make_async_copy(down_hbm.at[:, half_at(True, out_ref.shape[1])], down_ref, sem)
    copy.start()
    copy.wait()
    out_ref[...] = jnp.dot(act_ref[...], down_ref[...], preferred_element_type=jnp.float32)


def expert_rows(rows, gate_weight, up_weight, down_weight, pairs):
    slots, half = rows.shape
    width = gate_weight.shape[0]
    up_weight, down_weight = in_hbm(up_weight, down_weight)
    part = shape((slots, width), jnp.float32)
    side = pltpu.VMEM((width, half), jnp.bfloat16)
    other = lax.ppermute(rows, "tp", pairs)
    gate_part, up_part = call(
        enter_kernel,
        "enter",
        (part, part),
        [VMEM, VMEM, HBM],
        (rows, gate_weight, up_weight),
        scratch=(side, pltpu.SemaphoreType.DMA),
        flops=4 * slots * half * width,
    )
    act, sent = call(
        leave_kernel,
        "leave",
        (shape((slots, width), jnp.bfloat16), shape((slots, half), jnp.bfloat16)),
        [VMEM, VMEM, HBM, HBM, VMEM, VMEM],
        (other, gate_weight, up_weight, down_weight, gate_part, up_part),
        scratch=(side, side, pltpu.SemaphoreType.DMA((2,))),
        flops=6 * slots * half * width,
    )
    arrived = lax.ppermute(sent, "tp", pairs)
    kept = call(
        close_kernel,
        "close",
        shape((slots, half), jnp.float32),
        [VMEM, HBM],
        (act, down_weight),
        scratch=(side, pltpu.SemaphoreType.DMA),
        flops=2 * slots * half * width,
    )
    return (kept + arrived.astype(jnp.float32)).astype(jnp.bfloat16)


def exchanged(array, axis):
    return lax.all_to_all(array, axis, split_axis=0, concat_axis=0, tiled=True)


def body(
    hidden,
    attn_gain,
    query_weight,
    rotary_weight,
    key_up,
    cache_latent,
    cache_rotary,
    lengths,
    value_up,
    out_weight,
    mixed_gain,
    moe_gain,
    expert_ids,
    route_logits,
    gate_weight,
    up_weight,
    down_weight,
    final_gain,
):
    group_rows, features = hidden.shape
    _, nope_width, latent_width = key_up.shape
    rotary_width = rotary_weight.shape[1]
    own_rows = cache_latent.shape[0]
    groups = lax.axis_size("ep")
    peers = lax.axis_size("tp")
    pairs = [(i, i ^ 1) for i in range(peers)]
    half = features // 2
    capacity = 2 * group_rows * expert_ids.shape[1] // groups
    slots = groups * capacity

    query, own_hidden, own_slots, columns, trig = front(
        hidden,
        attn_gain,
        query_weight,
        rotary_weight,
        key_up[0],
        expert_ids,
        route_logits,
        lengths,
        peers,
        capacity,
    )
    query = exchanged(query, "tp")
    score_scale = (nope_width + rotary_width) ** (-0.5)
    out_latent = attend(query, trig, cache_latent, cache_rotary, lengths, score_scale)
    out_latent = exchanged(out_latent, "tp").reshape(group_rows, latent_width)
    head_out = jnp.dot(out_latent, value_up[0], preferred_element_type=jnp.float32)
    head_terms = jnp.dot(
        head_out.astype(jnp.bfloat16), out_weight, preferred_element_type=jnp.float32
    )
    head_terms = head_terms.astype(jnp.bfloat16).reshape(peers, own_rows, features)
    head_terms = exchanged(head_terms, "tp").reshape(group_rows, features)
    mixed_rows, normed = mix(head_terms, own_hidden, mixed_gain, moe_gain, peers)
    normed = exchanged(normed, "tp").reshape(group_rows, half)
    outgoing = dispatch(own_slots, normed, slots).reshape(groups, capacity, half)
    arrived = exchanged(outgoing, "ep").reshape(slots, half)
    result = expert_rows(arrived, gate_weight[0].T, up_weight[0].T, down_weight[0], pairs)
    returned = exchanged(result.reshape(groups, capacity, half), "ep").reshape(slots, half)
    combined = combine(columns, returned).reshape(peers, own_rows, half)
    terms = exchanged(combined, "tp").reshape(group_rows, half)
    return finish(terms, mixed_rows, final_gain)


def solution(mesh):
    placed = (
        P("ep", None),
        P(),
        P(None, "tp"),
        P(None, "tp"),
        P("tp", None, None),
        P(("ep", "tp"), None, None),
        P(("ep", "tp"), None, None),
        P(("ep", "tp")),
        P("tp", None, None),
        P("tp", None),
        P(),
        P(),
        P(),
        P(),
        P("ep", None, "tp"),
        P("ep", None, "tp"),
        P("ep", "tp", None),
        P(),
    )
    return jax.shard_map(
        body, mesh=mesh, in_specs=placed, out_specs=P(("ep", "tp"), None), check_vma=False
    )
```

```python
import functools

import jax
import jax.numpy as jnp
import numpy as np
from jax import lax
from jax.experimental import pallas as pl
from jax.experimental.pallas import tpu as pltpu
from jax.sharding import PartitionSpec as P

EPSILON = 1e-06
BLOCK = 1024
NEG = float("-inf")
VMEM = pl.BlockSpec(memory_space=pltpu.VMEM)
SMEM = pl.BlockSpec(memory_space=pltpu.SMEM)
HBM = pl.BlockSpec(memory_space=pltpu.HBM)
AHEAD = 10**10
ATTEND_LIMIT = 2 * 1024 * 1024
SMALL_LIMIT = 4 * 1024 * 1024
NT = (((1,), (1,)), ((), ()))


def call(kernel, name, outs, ins, args, scratch=(), limit=SMALL_LIMIT, flops=0):
    return pl.pallas_call(
        kernel,
        out_shape=outs,
        in_specs=ins,
        out_specs=jax.tree.map(lambda _: VMEM, outs),
        scratch_shapes=list(scratch),
        compiler_params=pltpu.CompilerParams(vmem_limit_bytes=limit),
        cost_estimate=pl.CostEstimate(flops=flops, bytes_accessed=0, transcendentals=0),
        name=name,
    )(*args)


def shape(dims, dtype):
    return jax.ShapeDtypeStruct(dims, dtype)


def norm_rows(values, gain_vector):
    values = values.astype(jnp.float32)
    factor = lax.rsqrt(jnp.mean(values * values, axis=-1, keepdims=True) + EPSILON)
    return values * factor * gain_vector


def column(row):
    size = row.shape[1]
    same = lax.broadcasted_iota(jnp.int32, (size, size), 0) == lax.broadcasted_iota(
        jnp.int32, (size, size), 1
    )
    return jnp.sum(jnp.where(same, row, 0.0), axis=1, keepdims=True)


def front_kernel(
    capacity, hidden_hbm, gain_hbm, query_hbm, rotary_hbm, key_hbm, ids_hbm, logits_hbm, lengths_hbm,
    out_ref, own_ref, slots_ref, columns_ref, trig_ref,
    hidden_ref, gain_ref, query_ref, rotary_ref, key_ref, ids_ref, logits_ref, lengths_ref, sems,
):
    group_rows, features = hidden_ref.shape
    peers, own_rows, _ = out_ref.shape
    latent = key_ref.shape[1]
    pairs = (
        (lengths_hbm, lengths_ref),
        (ids_hbm, ids_ref),
        (logits_hbm, logits_ref),
        (hidden_hbm, hidden_ref),
        (gain_hbm, gain_ref),
        (query_hbm, query_ref),
        (rotary_hbm, rotary_ref),
        (key_hbm, key_ref),
    )
    copies = [pltpu.make_async_copy(s, d, sems.at[i]) for i, (s, d) in enumerate(pairs)]
    for copy in copies:
        copy.start()
    group, place = lax.axis_index("ep"), lax.axis_index("tp")

    copies[1].wait()
    copies[2].wait()
    ids_all = ids_ref[...].astype(jnp.float32)
    logits_all = logits_ref[...]
    ids = jnp.zeros((2, group_rows), jnp.float32)
    logits = jnp.zeros((2, group_rows), jnp.float32)
    for g in range(ids_all.shape[1] // group_rows):
        at = slice(g * group_rows, (g + 1) * group_rows)
        ids = jnp.where(group == g, ids_all[:, at], ids)
        logits = jnp.where(group == g, logits_all[:, at], logits)
    id_rows = [ids[k : k + 1, :] for k in range(2)]
    id_columns = [column(row) for row in id_rows]
    before = lax.broadcasted_iota(jnp.int32, (group_rows, group_rows), 0) < lax.broadcasted_iota(
        jnp.int32, (group_rows, group_rows), 1
    )
    top = jnp.maximum(logits[0:1, :], logits[1:2, :])
    weights = [jnp.exp(logits[k : k + 1, :] - top) for k in range(2)]
    for k in range(2):
        hits = jnp.where(before & (id_columns[0] == id_rows[k]), 1.0, 0.0)
        hits = hits + jnp.where(before & (id_columns[1] == id_rows[k]), 1.0, 0.0)
        slot = id_rows[k] * capacity + jnp.sum(hits, axis=0, keepdims=True)
        slots_ref[k : k + 1, :] = slot
        columns_ref[:, k : k + 1] = column(slot)
        columns_ref[:, 2 + k : 3 + k] = column(weights[k] / (weights[0] + weights[1]))

    copies[0].wait()
    half = trig_ref.shape[1] // 2
    lane = lax.broadcasted_iota(jnp.int32, (1, 2 * half), 1)
    inverse = jnp.zeros((1, 2 * half), jnp.float32)
    for i in range(half):
        value = float(np.float32(10000.0 ** (-i / half)))
        inverse = jnp.where((lane == i) | (lane == i + half), value, inverse)
    for s in range(own_rows):
        angles = (lengths_ref[s] - 1).astype(jnp.float32) * inverse
        turned = jnp.sin(angles)
        trig_ref[2 * s : 2 * s + 1, :] = jnp.cos(angles)
        trig_ref[2 * s + 1 : 2 * s + 2, :] = jnp.where(lane < half, -turned, turned)
        at = 2 * own_rows + s
        trig_ref[at : at + 1, :] = jnp.zeros_like(angles) + lengths_ref[s].astype(jnp.float32)

    copies[3].wait()
    copies[4].wait()
    hidden = hidden_ref[...]
    normed = norm_rows(hidden, gain_ref[...]).astype(jnp.bfloat16)
    pick_row = lax.broadcasted_iota(jnp.int32, (8, group_rows), 0) + place * own_rows
    pick = jnp.where(pick_row == lax.broadcasted_iota(jnp.int32, (8, group_rows), 1), 1.0, 0.0)
    own = jnp.dot(pick.astype(jnp.bfloat16), hidden, preferred_element_type=jnp.float32)
    own_ref[...] = own[:own_rows].astype(jnp.bfloat16)
    copies[5].wait()
    copies[6].wait()
    copies[7].wait()
    nope = lax.dot_general(
        normed, query_ref[...], NT, preferred_element_type=jnp.float32
    ).astype(jnp.bfloat16)
    turned = lax.dot_general(normed, rotary_ref[...], NT, preferred_element_type=jnp.float32)
    projected = jnp.dot(nope, key_ref[...], preferred_element_type=jnp.float32)
    for t in range(peers):
        at = slice(t * own_rows, (t + 1) * own_rows)
        out_ref[t, :, :latent] = projected[at].astype(jnp.bfloat16)
        out_ref[t, :, latent:] = turned[at].astype(jnp.bfloat16)


def in_hbm(*arrays):
    return tuple(pltpu.with_memory_space_constraint(a, pltpu.HBM) for a in arrays)


def front(
    hidden, gain, query_weight, rotary_weight, key_up, ids, logits, lengths, peers, capacity,
):
    rows, features = hidden.shape
    own_rows = rows // peers
    rope, latent = rotary_weight.shape[1], key_up.shape[1]
    arrays = in_hbm(
        hidden, gain[None, :], query_weight.T, rotary_weight.T, key_up, ids.T, logits.T, lengths
    )
    held = [pltpu.VMEM(a.shape, a.dtype) for a in arrays[:-1]]
    return call(
        functools.partial(front_kernel, capacity),
        "front",
        (
            shape((peers, own_rows, latent + rope), jnp.bfloat16),
            shape((own_rows, features), jnp.bfloat16),
            shape((2, rows), jnp.float32),
            shape((rows, 4), jnp.float32),
            shape((3 * own_rows, rope), jnp.float32),
        ),
        [HBM] * 8,
        arrays,
        scratch=held + [pltpu.SMEM(lengths.shape, lengths.dtype), pltpu.SemaphoreType.DMA((8,))],
        flops=AHEAD,
    )


def attend_kernel(
    scale, query_ref, trig_ref, latent_ref, rope_ref, out_ref, latent_query, rotary_query, summed_ref
):
    rows, heads, width = latent_query.shape
    rope = rotary_query.shape[2]
    most = latent_ref.shape[1] // BLOCK
    lengths = [
        jnp.max(trig_ref[2 * rows + s : 2 * rows + s + 1, :]).astype(jnp.int32) for s in range(rows)
    ]
    counts = [lax.div(length + (BLOCK - 1), BLOCK) for length in lengths]

    place = lax.broadcasted_iota(jnp.int32, (rows * heads, rows * heads), 0)
    other = lax.broadcasted_iota(jnp.int32, (rows * heads, rows * heads), 1)
    by_head = jnp.where(lax.rem(place, rows) * heads + lax.div(place, rows) == other, 1.0, 0.0)
    swap = lax.broadcasted_iota(jnp.int32, (rope, rope), 0) == lax.rem(
        lax.broadcasted_iota(jnp.int32, (rope, rope), 1) + rope // 2, rope
    )
    swap = jnp.where(swap, 1.0, 0.0).astype(jnp.bfloat16)
    received = query_ref[...].astype(jnp.float32)
    query = jnp.concatenate(
        [received[h, s : s + 1, :] for s in range(rows) for h in range(heads)], axis=0
    )
    plain = query[:, width:]
    turned = jnp.dot(plain.astype(jnp.bfloat16), swap, preferred_element_type=jnp.float32)
    for s in range(rows):
        at = slice(s * heads, (s + 1) * heads)
        latent_query[s] = query[at, :width].astype(jnp.bfloat16)
        rotary_query[s] = (
            plain[at] * trig_ref[2 * s : 2 * s + 1, :]
            + turned[at] * trig_ref[2 * s + 1 : 2 * s + 2, :]
        ).astype(jnp.bfloat16)

    first = jnp.where(counts[0] <= counts[1], 0, 1)

    @pl.loop(0, rows)
    def _sequence(i):
        s = jnp.where(i == 0, first, 1 - first)
        length = jnp.where(s == 0, lengths[0], lengths[1])
        blocks = lax.div(length + (BLOCK - 1), BLOCK)
        for count in range(1, most + 1):

            @pl.when(blocks == count)
            def _attend(count=count):
                scores = []
                for b in range(count):
                    at = slice(b * BLOCK, (b + 1) * BLOCK)
                    part = lax.dot_general(
                        latent_query[s], latent_ref[s, at, :], NT,
                        preferred_element_type=jnp.float32,
                    )
                    part = part + jnp.dot(
                        rotary_query[s], rope_ref[s, :, at],
                        preferred_element_type=jnp.float32,
                    )
                    part = part * scale
                    if b == count - 1:
                        places = b * BLOCK + lax.broadcasted_iota(jnp.int32, (heads, BLOCK), 1)
                        part = jnp.where(places < length, part, NEG)
                    scores.append(part)
                highest = scores[0]
                for part in scores[1:]:
                    highest = jnp.maximum(highest, part)
                highest = jnp.max(highest, axis=1, keepdims=True)
                weights = [jnp.exp(part - highest) for part in scores]
                total = weights[0]
                for part in weights[1:]:
                    total = total + part
                factor = 1.0 / jnp.sum(total, axis=1, keepdims=True)
                summed = None
                for b in range(count):
                    probs = (weights[b] * factor).astype(jnp.bfloat16)
                    at = slice(b * BLOCK, (b + 1) * BLOCK)
                    term = jnp.dot(
                        probs, latent_ref[s, at, :],
                        preferred_element_type=jnp.float32,
                    )
                    summed = term if summed is None else summed + term
                summed_ref[s] = summed.astype(jnp.bfloat16)

    sums = jnp.concatenate([summed_ref[s] for s in range(rows)], axis=0)
    out_ref[...] = jnp.dot(
        by_head.astype(jnp.bfloat16), sums, preferred_element_type=jnp.float32
    ).astype(jnp.bfloat16)


def attend(query, trig, latent, rotary, scale):
    rows, most, width = latent.shape
    heads, rope = query.shape[0], rotary.shape[1]
    return call(
        functools.partial(attend_kernel, scale),
        "attend",
        shape((heads * rows, width), jnp.bfloat16),
        [VMEM] * 4,
        (query, trig, latent, rotary),
        scratch=(
            pltpu.VMEM((rows, heads, width), jnp.bfloat16),
            pltpu.VMEM((rows, heads, rope), jnp.bfloat16),
            pltpu.VMEM((rows, heads, width), jnp.bfloat16),
        ),
        limit=ATTEND_LIMIT,
        flops=4 * latent.size * heads,
    )


def row_sums(terms, rows, keep):
    place = lax.broadcasted_iota(jnp.int32, (8, terms.shape[0]), 1)
    wanted = (lax.rem(place, rows) == lax.broadcasted_iota(jnp.int32, place.shape, 0)) & keep(place)
    ones = jnp.where(wanted, 1.0, 0.0).astype(jnp.bfloat16)
    return jnp.dot(ones, terms, preferred_element_type=jnp.float32)


def mix_kernel(terms_ref, own_ref, mixed_gain_ref, moe_gain_ref, mixed_ref, send_ref):
    peers, rows, half = send_ref.shape
    attended = row_sums(terms_ref[...], rows, lambda place: place >= 0)[:rows].astype(jnp.bfloat16)
    mixed = (
        own_ref[...].astype(jnp.float32) + norm_rows(attended, mixed_gain_ref[...])
    ).astype(jnp.bfloat16)
    mixed_ref[...] = mixed
    normed = norm_rows(mixed, moe_gain_ref[...]).astype(jnp.bfloat16)
    for t in range(peers):
        send_ref[t] = normed[:, (t % 2) * half : (t % 2 + 1) * half]


def mix(terms, own, mixed_gain, moe_gain, peers):
    rows, features = own.shape
    return call(
        mix_kernel,
        "mix",
        (
            shape((rows, features), jnp.bfloat16),
            shape((peers, rows, features // 2), jnp.bfloat16),
        ),
        [VMEM] * 4,
        (terms, own, mixed_gain[None, :], moe_gain[None, :]),
    )


def dispatch_kernel(slots_ref, rows_ref, out_ref):
    slots, rows = out_ref.shape[0], rows_ref.shape[0]
    place = lax.broadcasted_iota(jnp.int32, (slots, rows), 0).astype(jnp.float32)
    taken = (place == slots_ref[0:1, :]) | (place == slots_ref[1:2, :])
    pick = jnp.where(taken, 1.0, 0.0).astype(jnp.bfloat16)
    out_ref[...] = jnp.dot(pick, rows_ref[...], preferred_element_type=jnp.float32).astype(
        jnp.bfloat16
    )


def dispatch(own_slots, rows, slots):
    return call(
        dispatch_kernel,
        "dispatch",
        shape((slots, rows.shape[1]), jnp.bfloat16),
        [VMEM] * 2,
        (own_slots, rows),
        flops=AHEAD,
    )


def combine_kernel(columns_ref, returned_ref, out_ref):
    rows, slots = out_ref.shape[0], returned_ref.shape[0]
    place = lax.broadcasted_iota(jnp.int32, (rows, slots), 1).astype(jnp.float32)
    gates = jnp.where(place == columns_ref[:, 0:1], columns_ref[:, 2:3], 0.0)
    gates = gates + jnp.where(place == columns_ref[:, 1:2], columns_ref[:, 3:4], 0.0)
    returned = returned_ref[...]
    total = None
    for _ in range(3):
        part = gates.astype(jnp.bfloat16)
        term = jnp.dot(part, returned, preferred_element_type=jnp.float32)
        total = term if total is None else total + term
        gates = gates - part.astype(jnp.float32)
    out_ref[...] = total.astype(jnp.bfloat16)


def combine(columns, returned):
    return call(
        combine_kernel,
        "combine",
        shape((columns.shape[0], returned.shape[1]), jnp.bfloat16),
        [VMEM] * 2,
        (columns, returned),
    )


def finish_kernel(terms_ref, mixed_ref, gain_ref, out_ref):
    rows = mixed_ref.shape[0]
    terms = terms_ref[...]
    halves = [
        row_sums(terms, rows, lambda place, c=c: lax.rem(lax.div(place, rows), 2) == c)
        for c in range(2)
    ]
    routed = jnp.concatenate(halves, axis=1)[:rows].astype(jnp.bfloat16)
    out_ref[...] = (
        mixed_ref[...].astype(jnp.float32) + norm_rows(routed, gain_ref[...])
    ).astype(jnp.bfloat16)


def finish(terms, mixed, gain):
    return call(
        finish_kernel,
        "finish",
        shape(mixed.shape, jnp.bfloat16),
        [VMEM] * 3,
        (terms, mixed, gain[None, :]),
    )


def half_at(own, half):
    core = lax.rem(lax.axis_index("tp"), 2)
    if not own:
        core = 1 - core
    return pl.ds(pl.multiple_of(core * half, half), half)


def product(rows, weight):
    return lax.dot_general(rows, weight, NT, preferred_element_type=jnp.float32)


def enter_kernel(rows_ref, gate_ref, up_ref, gate_out, up_out):
    rows = rows_ref[...]
    at = half_at(True, rows.shape[1])
    gate_out[...] = product(rows, gate_ref[:, at])
    up_out[...] = product(rows, up_ref[:, at])


def leave_kernel(rows_ref, gate_ref, up_ref, down_ref, gate_part, up_part, act_ref, out_ref):
    rows = rows_ref[...]
    at = half_at(False, rows.shape[1])
    gate = gate_part[...] + product(rows, gate_ref[:, at])
    up = up_part[...] + product(rows, up_ref[:, at])
    act = (gate / (1.0 + jnp.exp(-gate)) * up).astype(jnp.bfloat16)
    act_ref[...] = act
    out_ref[...] = jnp.dot(act, down_ref[:, at], preferred_element_type=jnp.float32).astype(
        jnp.bfloat16
    )


def close_kernel(act_ref, down_ref, out_ref):
    at = half_at(True, out_ref.shape[1])
    out_ref[...] = jnp.dot(act_ref[...], down_ref[:, at], preferred_element_type=jnp.float32)


def expert_rows(rows, gate_weight, up_weight, down_weight, pairs):
    slots, half = rows.shape
    width = gate_weight.shape[0]
    part = shape((slots, width), jnp.float32)
    other = lax.ppermute(rows, "tp", pairs)
    gate_part, up_part = call(
        enter_kernel,
        "enter",
        (part, part),
        [VMEM] * 3,
        (rows, gate_weight, up_weight),
        flops=4 * slots * half * width,
    )
    act, sent = call(
        leave_kernel,
        "leave",
        (shape((slots, width), jnp.bfloat16), shape((slots, half), jnp.bfloat16)),
        [VMEM] * 6,
        (other, gate_weight, up_weight, down_weight, gate_part, up_part),
        flops=6 * slots * half * width,
    )
    arrived = lax.ppermute(sent, "tp", pairs)
    kept = call(
        close_kernel,
        "close",
        shape((slots, half), jnp.float32),
        [VMEM] * 2,
        (act, down_weight),
        flops=2 * slots * half * width,
    )
    return (kept + arrived.astype(jnp.float32)).astype(jnp.bfloat16)


def exchanged(array, axis):
    return lax.all_to_all(array, axis, split_axis=0, concat_axis=0, tiled=True)


def body(
    hidden,
    attn_gain,
    query_weight,
    rotary_weight,
    key_up,
    cache_latent,
    cache_rotary,
    lengths,
    value_up,
    out_weight,
    mixed_gain,
    moe_gain,
    expert_ids,
    route_logits,
    gate_weight,
    up_weight,
    down_weight,
    final_gain,
):
    group_rows, features = hidden.shape
    _, nope_width, latent_width = key_up.shape
    rotary_width = rotary_weight.shape[1]
    own_rows = cache_latent.shape[0]
    groups = lax.axis_size("ep")
    peers = lax.axis_size("tp")
    pairs = [(i, i ^ 1) for i in range(peers)]
    half = features // 2
    capacity = 2 * group_rows * expert_ids.shape[1] // groups
    slots = groups * capacity

    query, own_hidden, own_slots, columns, trig = front(
        hidden,
        attn_gain,
        query_weight,
        rotary_weight,
        key_up[0],
        expert_ids,
        route_logits,
        lengths,
        peers,
        capacity,
    )
    query = exchanged(query, "tp")
    score_scale = (nope_width + rotary_width) ** (-0.5)
    out_latent = attend(
        query, trig, cache_latent, cache_rotary, score_scale
    )
    out_latent = exchanged(out_latent.reshape(peers, own_rows, latent_width), "tp")
    out_latent = out_latent.reshape(group_rows, latent_width)
    head_out = jnp.dot(out_latent, value_up[0], preferred_element_type=jnp.float32)
    head_terms = jnp.dot(
        head_out.astype(jnp.bfloat16), out_weight, preferred_element_type=jnp.float32
    )
    head_terms = head_terms.astype(jnp.bfloat16).reshape(peers, own_rows, features)
    head_terms = exchanged(head_terms, "tp").reshape(group_rows, features)
    mixed_rows, normed = mix(head_terms, own_hidden, mixed_gain, moe_gain, peers)
    normed = exchanged(normed, "tp").reshape(group_rows, half)
    outgoing = dispatch(own_slots, normed, slots).reshape(groups, capacity, half)
    arrived = exchanged(outgoing, "ep").reshape(slots, half)
    result = expert_rows(arrived, gate_weight[0].T, up_weight[0].T, down_weight[0], pairs)
    returned = exchanged(result.reshape(groups, capacity, half), "ep").reshape(slots, half)
    combined = combine(columns, returned).reshape(peers, own_rows, half)
    terms = exchanged(combined, "tp").reshape(group_rows, half)
    return finish(terms, mixed_rows, final_gain)


def solution(mesh):
    placed = (
        P("ep", None),
        P(),
        P(None, "tp"),
        P(None, "tp"),
        P("tp", None, None),
        P(("ep", "tp"), None, None),
        P(("ep", "tp"), None, None),
        P(("ep", "tp")),
        P("tp", None, None),
        P("tp", None),
        P(),
        P(),
        P(),
        P(),
        P("ep", None, "tp"),
        P("ep", None, "tp"),
        P("ep", "tp", None),
        P(),
    )
    return jax.shard_map(
        body, mesh=mesh, in_specs=placed, out_specs=P(("ep", "tp"), None), check_vma=False
    )
```

```python
import functools

import jax
import jax.numpy as jnp
import numpy as np
from jax import lax
from jax.experimental import pallas as pl
from jax.experimental.pallas import tpu as pltpu
from jax.sharding import PartitionSpec as P

EPSILON = 1e-06
BLOCK = 1024
NEG = float("-inf")
VMEM = pl.BlockSpec(memory_space=pltpu.VMEM)
SMEM = pl.BlockSpec(memory_space=pltpu.SMEM)
HBM = pl.BlockSpec(memory_space=pltpu.HBM)
AHEAD = 10**10
ATTEND_LIMIT = 2 * 1024 * 1024
SMALL_LIMIT = 4 * 1024 * 1024
NT = (((1,), (1,)), ((), ()))


def call(kernel, name, outs, ins, args, scratch=(), limit=SMALL_LIMIT, flops=0):
    return pl.pallas_call(
        kernel,
        out_shape=outs,
        in_specs=ins,
        out_specs=jax.tree.map(lambda _: VMEM, outs),
        scratch_shapes=list(scratch),
        compiler_params=pltpu.CompilerParams(vmem_limit_bytes=limit),
        cost_estimate=pl.CostEstimate(flops=flops, bytes_accessed=0, transcendentals=0),
        name=name,
    )(*args)


def shape(dims, dtype):
    return jax.ShapeDtypeStruct(dims, dtype)


def norm_rows(values, gain_vector):
    values = values.astype(jnp.float32)
    factor = lax.rsqrt(jnp.mean(values * values, axis=-1, keepdims=True) + EPSILON)
    return values * factor * gain_vector


def column(row):
    size = row.shape[1]
    same = lax.broadcasted_iota(jnp.int32, (size, size), 0) == lax.broadcasted_iota(
        jnp.int32, (size, size), 1
    )
    return jnp.sum(jnp.where(same, row, 0.0), axis=1, keepdims=True)


def front_kernel(
    capacity, hidden_hbm, gain_hbm, query_hbm, rotary_hbm, key_hbm, ids_hbm, logits_hbm, lengths_hbm,
    out_ref, own_ref, slots_ref, columns_ref, trig_ref,
    hidden_ref, gain_ref, query_ref, rotary_ref, key_ref, ids_ref, logits_ref, lengths_ref, sems,
):
    group_rows, features = hidden_ref.shape
    peers, own_rows, _ = out_ref.shape
    latent = key_ref.shape[1]
    pairs = (
        (lengths_hbm, lengths_ref),
        (ids_hbm, ids_ref),
        (logits_hbm, logits_ref),
        (hidden_hbm, hidden_ref),
        (gain_hbm, gain_ref),
        (query_hbm, query_ref),
        (rotary_hbm, rotary_ref),
        (key_hbm, key_ref),
    )
    copies = [pltpu.make_async_copy(s, d, sems.at[i]) for i, (s, d) in enumerate(pairs)]
    for copy in copies:
        copy.start()
    group, place = lax.axis_index("ep"), lax.axis_index("tp")
    for copy in copies:
        copy.wait()
    ids_all = ids_ref[...].astype(jnp.float32)
    logits_all = logits_ref[...]
    ids = jnp.zeros((2, group_rows), jnp.float32)
    logits = jnp.zeros((2, group_rows), jnp.float32)
    for g in range(ids_all.shape[1] // group_rows):
        at = slice(g * group_rows, (g + 1) * group_rows)
        ids = jnp.where(group == g, ids_all[:, at], ids)
        logits = jnp.where(group == g, logits_all[:, at], logits)
    id_rows = [ids[k : k + 1, :] for k in range(2)]
    id_columns = [column(row) for row in id_rows]
    before = lax.broadcasted_iota(jnp.int32, (group_rows, group_rows), 0) < lax.broadcasted_iota(
        jnp.int32, (group_rows, group_rows), 1
    )
    top = jnp.maximum(logits[0:1, :], logits[1:2, :])
    weights = [jnp.exp(logits[k : k + 1, :] - top) for k in range(2)]
    for k in range(2):
        hits = jnp.where(before & (id_columns[0] == id_rows[k]), 1.0, 0.0)
        hits = hits + jnp.where(before & (id_columns[1] == id_rows[k]), 1.0, 0.0)
        slot = id_rows[k] * capacity + jnp.sum(hits, axis=0, keepdims=True)
        slots_ref[k : k + 1, :] = slot
        columns_ref[:, k : k + 1] = column(slot)
        columns_ref[:, 2 + k : 3 + k] = column(weights[k] / (weights[0] + weights[1]))

    half = trig_ref.shape[1] // 2
    lane = lax.broadcasted_iota(jnp.int32, (1, 2 * half), 1)
    inverse = jnp.zeros((1, 2 * half), jnp.float32)
    for i in range(half):
        value = float(np.float32(10000.0 ** (-i / half)))
        inverse = jnp.where((lane == i) | (lane == i + half), value, inverse)
    for s in range(own_rows):
        angles = (lengths_ref[s] - 1).astype(jnp.float32) * inverse
        turned = jnp.sin(angles)
        trig_ref[2 * s : 2 * s + 1, :] = jnp.cos(angles)
        trig_ref[2 * s + 1 : 2 * s + 2, :] = jnp.where(lane < half, -turned, turned)
        at = 2 * own_rows + s
        trig_ref[at : at + 1, :] = jnp.zeros_like(angles) + lengths_ref[s].astype(jnp.float32)

    hidden = hidden_ref[...]
    normed = norm_rows(hidden, gain_ref[...]).astype(jnp.bfloat16)
    pick_row = lax.broadcasted_iota(jnp.int32, (8, group_rows), 0) + place * own_rows
    pick = jnp.where(pick_row == lax.broadcasted_iota(jnp.int32, (8, group_rows), 1), 1.0, 0.0)
    own = jnp.dot(pick.astype(jnp.bfloat16), hidden, preferred_element_type=jnp.float32)
    own_ref[...] = own[:own_rows].astype(jnp.bfloat16)
    nope = lax.dot_general(
        normed, query_ref[...], NT, preferred_element_type=jnp.float32
    ).astype(jnp.bfloat16)
    turned = lax.dot_general(normed, rotary_ref[...], NT, preferred_element_type=jnp.float32)
    projected = jnp.dot(nope, key_ref[...], preferred_element_type=jnp.float32)
    for t in range(peers):
        at = slice(t * own_rows, (t + 1) * own_rows)
        out_ref[t, :, :latent] = projected[at].astype(jnp.bfloat16)
        out_ref[t, :, latent:] = turned[at].astype(jnp.bfloat16)


def in_hbm(*arrays):
    return tuple(pltpu.with_memory_space_constraint(a, pltpu.HBM) for a in arrays)


def front(
    hidden, gain, query_weight, rotary_weight, key_up, ids, logits, lengths, peers, capacity,
):
    rows, features = hidden.shape
    own_rows = rows // peers
    rope, latent = rotary_weight.shape[1], key_up.shape[1]
    arrays = in_hbm(
        hidden, gain[None, :], query_weight.T, rotary_weight.T, key_up, ids.T, logits.T, lengths
    )
    held = [pltpu.VMEM(a.shape, a.dtype) for a in arrays[:-1]]
    return call(
        functools.partial(front_kernel, capacity),
        "front",
        (
            shape((peers, own_rows, latent + rope), jnp.bfloat16),
            shape((own_rows, features), jnp.bfloat16),
            shape((2, rows), jnp.float32),
            shape((rows, 4), jnp.float32),
            shape((3 * own_rows, rope), jnp.float32),
        ),
        [HBM] * 8,
        arrays,
        scratch=held + [pltpu.SMEM(lengths.shape, lengths.dtype), pltpu.SemaphoreType.DMA((8,))],
        flops=AHEAD,
    )


def attend_kernel(
    scale, query_ref, trig_ref, latent_ref, rope_ref, out_ref, latent_query, rotary_query, summed_ref
):
    rows, heads, width = latent_query.shape
    rope = rotary_query.shape[2]
    most = latent_ref.shape[1] // BLOCK
    lengths = [
        jnp.max(trig_ref[2 * rows + s : 2 * rows + s + 1, :]).astype(jnp.int32) for s in range(rows)
    ]
    counts = [lax.div(length + (BLOCK - 1), BLOCK) for length in lengths]

    place = lax.broadcasted_iota(jnp.int32, (rows * heads, rows * heads), 0)
    other = lax.broadcasted_iota(jnp.int32, (rows * heads, rows * heads), 1)
    by_head = jnp.where(lax.rem(place, rows) * heads + lax.div(place, rows) == other, 1.0, 0.0)
    swap = lax.broadcasted_iota(jnp.int32, (rope, rope), 0) == lax.rem(
        lax.broadcasted_iota(jnp.int32, (rope, rope), 1) + rope // 2, rope
    )
    swap = jnp.where(swap, 1.0, 0.0).astype(jnp.bfloat16)
    received = query_ref[...].astype(jnp.float32)
    query = jnp.concatenate(
        [received[h, s : s + 1, :] for s in range(rows) for h in range(heads)], axis=0
    )
    plain = query[:, width:]
    turned = jnp.dot(plain.astype(jnp.bfloat16), swap, preferred_element_type=jnp.float32)
    for s in range(rows):
        at = slice(s * heads, (s + 1) * heads)
        latent_query[s] = query[at, :width].astype(jnp.bfloat16)
        rotary_query[s] = (
            plain[at] * trig_ref[2 * s : 2 * s + 1, :]
            + turned[at] * trig_ref[2 * s + 1 : 2 * s + 2, :]
        ).astype(jnp.bfloat16)

    larger = jnp.where(counts[0] >= counts[1], 0, 1)
    order = (larger, 1 - larger)
    ordered = [jnp.where(s == 0, lengths[0], lengths[1]) for s in order]
    large, small = [lax.div(length + (BLOCK - 1), BLOCK) for length in ordered]

    def score(s, length, b, last):
        at = slice(b * BLOCK, (b + 1) * BLOCK)
        part = product(latent_query[s], latent_ref[s, at, :])
        part = part + jnp.dot(
            rotary_query[s], rope_ref[s, :, at], preferred_element_type=jnp.float32
        )
        part = part * scale
        if last:
            places = b * BLOCK + lax.broadcasted_iota(jnp.int32, (heads, BLOCK), 1)
            part = jnp.where(places < length, part, NEG)
        return part

    def soften(scores):
        highest = functools.reduce(jnp.maximum, scores)
        highest = jnp.max(highest, axis=1, keepdims=True)
        weights = [jnp.exp(part - highest) for part in scores]
        total = functools.reduce(jnp.add, weights)
        factor = 1.0 / jnp.sum(total, axis=1, keepdims=True)
        return [(part * factor).astype(jnp.bfloat16) for part in weights]

    def weigh(s, probs):
        terms = [
            jnp.dot(
                part, latent_ref[s, b * BLOCK : (b + 1) * BLOCK, :],
                preferred_element_type=jnp.float32,
            )
            for b, part in enumerate(probs)
        ]
        summed_ref[s] = functools.reduce(jnp.add, terms).astype(jnp.bfloat16)

    for most_blocks in range(1, most + 1):
        for least_blocks in range(1, most_blocks + 1):

            @pl.when((large == most_blocks) & (small == least_blocks))
            def _attend(filled=(most_blocks, least_blocks)):
                scores = [
                    [score(s, length, b, b == count - 1) for b in range(count)]
                    for s, length, count in zip(order, ordered, filled)
                ]
                for s, parts in zip(order, scores):
                    weigh(s, soften(parts))

    sums = jnp.concatenate([summed_ref[s] for s in range(rows)], axis=0)
    out_ref[...] = jnp.dot(
        by_head.astype(jnp.bfloat16), sums, preferred_element_type=jnp.float32
    ).astype(jnp.bfloat16)


def attend(query, trig, latent, rotary, scale):
    rows, most, width = latent.shape
    heads, rope = query.shape[0], rotary.shape[1]
    return call(
        functools.partial(attend_kernel, scale),
        "attend",
        shape((heads * rows, width), jnp.bfloat16),
        [VMEM] * 4,
        (query, trig, latent, rotary),
        scratch=(
            pltpu.VMEM((rows, heads, width), jnp.bfloat16),
            pltpu.VMEM((rows, heads, rope), jnp.bfloat16),
            pltpu.VMEM((rows, heads, width), jnp.bfloat16),
        ),
        limit=ATTEND_LIMIT,
        flops=4 * latent.size * heads,
    )


def row_sums(terms, rows, keep):
    place = lax.broadcasted_iota(jnp.int32, (8, terms.shape[0]), 1)
    wanted = (lax.rem(place, rows) == lax.broadcasted_iota(jnp.int32, place.shape, 0)) & keep(place)
    ones = jnp.where(wanted, 1.0, 0.0).astype(jnp.bfloat16)
    return jnp.dot(ones, terms, preferred_element_type=jnp.float32)


def mix_kernel(terms_ref, own_ref, mixed_gain_ref, moe_gain_ref, mixed_ref, send_ref):
    peers, rows, half = send_ref.shape
    attended = row_sums(terms_ref[...], rows, lambda place: place >= 0)[:rows].astype(jnp.bfloat16)
    mixed = (
        own_ref[...].astype(jnp.float32) + norm_rows(attended, mixed_gain_ref[...])
    ).astype(jnp.bfloat16)
    mixed_ref[...] = mixed
    normed = norm_rows(mixed, moe_gain_ref[...]).astype(jnp.bfloat16)
    for t in range(peers):
        send_ref[t] = normed[:, (t % 2) * half : (t % 2 + 1) * half]


def mix(terms, own, mixed_gain, moe_gain, peers):
    rows, features = own.shape
    return call(
        mix_kernel,
        "mix",
        (
            shape((rows, features), jnp.bfloat16),
            shape((peers, rows, features // 2), jnp.bfloat16),
        ),
        [VMEM] * 4,
        (terms, own, mixed_gain[None, :], moe_gain[None, :]),
    )


def dispatch_kernel(slots_ref, rows_ref, out_ref):
    slots, rows = out_ref.shape[0], rows_ref.shape[0]
    place = lax.broadcasted_iota(jnp.int32, (slots, rows), 0).astype(jnp.float32)
    taken = (place == slots_ref[0:1, :]) | (place == slots_ref[1:2, :])
    pick = jnp.where(taken, 1.0, 0.0).astype(jnp.bfloat16)
    out_ref[...] = jnp.dot(pick, rows_ref[...], preferred_element_type=jnp.float32).astype(
        jnp.bfloat16
    )


def dispatch(own_slots, rows, slots):
    return call(
        dispatch_kernel,
        "dispatch",
        shape((slots, rows.shape[1]), jnp.bfloat16),
        [VMEM] * 2,
        (own_slots, rows),
        flops=AHEAD,
    )


def combine_kernel(columns_ref, returned_ref, out_ref):
    rows, slots = out_ref.shape[0], returned_ref.shape[0]
    place = lax.broadcasted_iota(jnp.int32, (rows, slots), 1).astype(jnp.float32)
    gates = jnp.where(place == columns_ref[:, 0:1], columns_ref[:, 2:3], 0.0)
    gates = gates + jnp.where(place == columns_ref[:, 1:2], columns_ref[:, 3:4], 0.0)
    returned = returned_ref[...]
    total = None
    for _ in range(3):
        part = gates.astype(jnp.bfloat16)
        term = jnp.dot(part, returned, preferred_element_type=jnp.float32)
        total = term if total is None else total + term
        gates = gates - part.astype(jnp.float32)
    out_ref[...] = total.astype(jnp.bfloat16)


def combine(columns, returned):
    return call(
        combine_kernel,
        "combine",
        shape((columns.shape[0], returned.shape[1]), jnp.bfloat16),
        [VMEM] * 2,
        (columns, returned),
    )


def finish_kernel(terms_ref, mixed_ref, gain_ref, out_ref):
    rows = mixed_ref.shape[0]
    terms = terms_ref[...]
    halves = [
        row_sums(terms, rows, lambda place, c=c: lax.rem(lax.div(place, rows), 2) == c)
        for c in range(2)
    ]
    routed = jnp.concatenate(halves, axis=1)[:rows].astype(jnp.bfloat16)
    out_ref[...] = (
        mixed_ref[...].astype(jnp.float32) + norm_rows(routed, gain_ref[...])
    ).astype(jnp.bfloat16)


def finish(terms, mixed, gain):
    return call(
        finish_kernel,
        "finish",
        shape(mixed.shape, jnp.bfloat16),
        [VMEM] * 3,
        (terms, mixed, gain[None, :]),
    )


def half_at(own, half):
    core = lax.rem(lax.axis_index("tp"), 2)
    if not own:
        core = 1 - core
    return pl.ds(pl.multiple_of(core * half, half), half)


def product(rows, weight):
    return lax.dot_general(rows, weight, NT, preferred_element_type=jnp.float32)


def enter_kernel(rows_ref, gate_ref, up_ref, down_ref, gate_out, up_out):
    del down_ref
    rows = rows_ref[...]
    at = half_at(True, rows.shape[1])
    gate_out[...] = product(rows, gate_ref[:, at])
    up_out[...] = product(rows, up_ref[:, at])


def leave_kernel(rows_ref, gate_ref, up_ref, down_ref, gate_part, up_part, act_ref, out_ref):
    rows = rows_ref[...]
    at = half_at(False, rows.shape[1])
    gate = gate_part[...] + product(rows, gate_ref[:, at])
    up = up_part[...] + product(rows, up_ref[:, at])
    act = (gate / (1.0 + jnp.exp(-gate)) * up).astype(jnp.bfloat16)
    act_ref[...] = act
    out_ref[...] = jnp.dot(act, down_ref[:, at], preferred_element_type=jnp.float32).astype(
        jnp.bfloat16
    )


def close_kernel(act_ref, down_ref, out_ref):
    at = half_at(True, out_ref.shape[1])
    out_ref[...] = jnp.dot(act_ref[...], down_ref[:, at], preferred_element_type=jnp.float32)


def expert_rows(rows, gate_weight, up_weight, down_weight, pairs):
    slots, half = rows.shape
    width = gate_weight.shape[0]
    part = shape((slots, width), jnp.float32)
    other = lax.ppermute(rows, "tp", pairs)
    gate_part, up_part = call(
        enter_kernel,
        "enter",
        (part, part),
        [VMEM] * 4,
        (rows, gate_weight, up_weight, down_weight),
        flops=4 * slots * half * width,
    )
    act, sent = call(
        leave_kernel,
        "leave",
        (shape((slots, width), jnp.bfloat16), shape((slots, half), jnp.bfloat16)),
        [VMEM] * 6,
        (other, gate_weight, up_weight, down_weight, gate_part, up_part),
        flops=6 * slots * half * width,
    )
    arrived = lax.ppermute(sent, "tp", pairs)
    kept = call(
        close_kernel,
        "close",
        shape((slots, half), jnp.float32),
        [VMEM] * 2,
        (act, down_weight),
        flops=2 * slots * half * width,
    )
    return (kept + arrived.astype(jnp.float32)).astype(jnp.bfloat16)


def exchanged(array, axis):
    return lax.all_to_all(array, axis, split_axis=0, concat_axis=0, tiled=True)


def body(
    hidden,
    attn_gain,
    query_weight,
    rotary_weight,
    key_up,
    cache_latent,
    cache_rotary,
    lengths,
    value_up,
    out_weight,
    mixed_gain,
    moe_gain,
    expert_ids,
    route_logits,
    gate_weight,
    up_weight,
    down_weight,
    final_gain,
):
    group_rows, features = hidden.shape
    _, nope_width, latent_width = key_up.shape
    rotary_width = rotary_weight.shape[1]
    own_rows = cache_latent.shape[0]
    groups = lax.axis_size("ep")
    peers = lax.axis_size("tp")
    pairs = [(i, i ^ 1) for i in range(peers)]
    half = features // 2
    capacity = 2 * group_rows * expert_ids.shape[1] // groups
    slots = groups * capacity

    query, own_hidden, own_slots, columns, trig = front(
        hidden,
        attn_gain,
        query_weight,
        rotary_weight,
        key_up[0],
        expert_ids,
        route_logits,
        lengths,
        peers,
        capacity,
    )
    query = exchanged(query, "tp")
    score_scale = (nope_width + rotary_width) ** (-0.5)
    out_latent = attend(
        query, trig, cache_latent, cache_rotary, score_scale
    )
    out_latent = exchanged(out_latent.reshape(peers, own_rows, latent_width), "tp")
    out_latent = out_latent.reshape(group_rows, latent_width)
    head_out = jnp.dot(out_latent, value_up[0], preferred_element_type=jnp.float32)
    head_terms = jnp.dot(
        head_out.astype(jnp.bfloat16), out_weight, preferred_element_type=jnp.float32
    )
    head_terms = head_terms.astype(jnp.bfloat16).reshape(peers, own_rows, features)
    head_terms = exchanged(head_terms, "tp").reshape(group_rows, features)
    mixed_rows, normed = mix(head_terms, own_hidden, mixed_gain, moe_gain, peers)
    normed = exchanged(normed, "tp").reshape(group_rows, half)
    outgoing = dispatch(own_slots, normed, slots).reshape(groups, capacity, half)
    arrived = exchanged(outgoing, "ep").reshape(slots, half)
    result = expert_rows(arrived, gate_weight[0].T, up_weight[0].T, down_weight[0], pairs)
    returned = exchanged(result.reshape(groups, capacity, half), "ep").reshape(slots, half)
    combined = combine(columns, returned).reshape(peers, own_rows, half)
    terms = exchanged(combined, "tp").reshape(group_rows, half)
    return finish(terms, mixed_rows, final_gain)


def solution(mesh):
    placed = (
        P("ep", None),
        P(),
        P(None, "tp"),
        P(None, "tp"),
        P("tp", None, None),
        P(("ep", "tp"), None, None),
        P(("ep", "tp"), None, None),
        P(("ep", "tp")),
        P("tp", None, None),
        P("tp", None),
        P(),
        P(),
        P(),
        P(),
        P("ep", None, "tp"),
        P("ep", None, "tp"),
        P("ep", "tp", None),
        P(),
    )
    return jax.shard_map(
        body, mesh=mesh, in_specs=placed, out_specs=P(("ep", "tp"), None), check_vma=False
    )
```

```python
import functools

import jax
import jax.numpy as jnp
import numpy as np
from jax import lax
from jax.experimental import pallas as pl
from jax.experimental.pallas import tpu as pltpu
from jax.sharding import PartitionSpec as P

EPSILON = 1e-06
BLOCK = 1024
NEG = float("-inf")
VMEM = pl.BlockSpec(memory_space=pltpu.VMEM)
SMEM = pl.BlockSpec(memory_space=pltpu.SMEM)
HBM = pl.BlockSpec(memory_space=pltpu.HBM)
AHEAD = 10**10
ATTEND_LIMIT = 2 * 1024 * 1024
SMALL_LIMIT = 4 * 1024 * 1024
NT = (((1,), (1,)), ((), ()))


def call(kernel, name, outs, ins, args, scratch=(), limit=SMALL_LIMIT, flops=0):
    return pl.pallas_call(
        kernel,
        out_shape=outs,
        in_specs=ins,
        out_specs=jax.tree.map(lambda _: VMEM, outs),
        scratch_shapes=list(scratch),
        compiler_params=pltpu.CompilerParams(vmem_limit_bytes=limit),
        cost_estimate=pl.CostEstimate(flops=flops, bytes_accessed=0, transcendentals=0),
        name=name,
    )(*args)


def shape(dims, dtype):
    return jax.ShapeDtypeStruct(dims, dtype)


def norm_rows(values, gain_vector):
    values = values.astype(jnp.float32)
    factor = lax.rsqrt(jnp.mean(values * values, axis=-1, keepdims=True) + EPSILON)
    return values * factor * gain_vector


def column(row):
    size = row.shape[1]
    same = lax.broadcasted_iota(jnp.int32, (size, size), 0) == lax.broadcasted_iota(
        jnp.int32, (size, size), 1
    )
    return jnp.sum(jnp.where(same, row, 0.0), axis=1, keepdims=True)


def front_kernel(
    capacity, hidden_hbm, gain_hbm, query_hbm, rotary_hbm, key_hbm, ids_hbm, logits_hbm, lengths_hbm,
    out_ref, own_ref, slots_ref, columns_ref, trig_ref,
    hidden_ref, gain_ref, query_ref, rotary_ref, key_ref, ids_ref, logits_ref, lengths_ref, sems,
):
    group_rows, features = hidden_ref.shape
    peers, own_rows, _ = out_ref.shape
    latent = key_ref.shape[1]
    pairs = (
        (lengths_hbm, lengths_ref),
        (ids_hbm, ids_ref),
        (logits_hbm, logits_ref),
        (hidden_hbm, hidden_ref),
        (gain_hbm, gain_ref),
        (query_hbm, query_ref),
        (rotary_hbm, rotary_ref),
        (key_hbm, key_ref),
    )
    copies = [pltpu.make_async_copy(s, d, sems.at[i]) for i, (s, d) in enumerate(pairs)]
    for copy in copies:
        copy.start()
    group, place = lax.axis_index("ep"), lax.axis_index("tp")
    for copy in copies:
        copy.wait()
    ids_all = ids_ref[...].astype(jnp.float32)
    logits_all = logits_ref[...]
    ids = jnp.zeros((2, group_rows), jnp.float32)
    logits = jnp.zeros((2, group_rows), jnp.float32)
    for g in range(ids_all.shape[1] // group_rows):
        at = slice(g * group_rows, (g + 1) * group_rows)
        ids = jnp.where(group == g, ids_all[:, at], ids)
        logits = jnp.where(group == g, logits_all[:, at], logits)
    id_rows = [ids[k : k + 1, :] for k in range(2)]
    id_columns = [column(row) for row in id_rows]
    before = lax.broadcasted_iota(jnp.int32, (group_rows, group_rows), 0) < lax.broadcasted_iota(
        jnp.int32, (group_rows, group_rows), 1
    )
    top = jnp.maximum(logits[0:1, :], logits[1:2, :])
    weights = [jnp.exp(logits[k : k + 1, :] - top) for k in range(2)]
    for k in range(2):
        hits = jnp.where(before & (id_columns[0] == id_rows[k]), 1.0, 0.0)
        hits = hits + jnp.where(before & (id_columns[1] == id_rows[k]), 1.0, 0.0)
        slot = id_rows[k] * capacity + jnp.sum(hits, axis=0, keepdims=True)
        slots_ref[k : k + 1, :] = slot
        columns_ref[:, k : k + 1] = column(slot)
        columns_ref[:, 2 + k : 3 + k] = column(weights[k] / (weights[0] + weights[1]))

    half = trig_ref.shape[1] // 2
    lane = lax.broadcasted_iota(jnp.int32, (1, 2 * half), 1)
    inverse = jnp.zeros((1, 2 * half), jnp.float32)
    for i in range(half):
        value = float(np.float32(10000.0 ** (-i / half)))
        inverse = jnp.where((lane == i) | (lane == i + half), value, inverse)
    for s in range(own_rows):
        angles = (lengths_ref[s] - 1).astype(jnp.float32) * inverse
        turned = jnp.sin(angles)
        trig_ref[2 * s : 2 * s + 1, :] = jnp.cos(angles)
        trig_ref[2 * s + 1 : 2 * s + 2, :] = jnp.where(lane < half, -turned, turned)
        at = 2 * own_rows + s
        trig_ref[at : at + 1, :] = jnp.zeros_like(angles) + lengths_ref[s].astype(jnp.float32)

    hidden = hidden_ref[...]
    normed = norm_rows(hidden, gain_ref[...]).astype(jnp.bfloat16)
    pick_row = lax.broadcasted_iota(jnp.int32, (8, group_rows), 0) + place * own_rows
    pick = jnp.where(pick_row == lax.broadcasted_iota(jnp.int32, (8, group_rows), 1), 1.0, 0.0)
    own = jnp.dot(pick.astype(jnp.bfloat16), hidden, preferred_element_type=jnp.float32)
    own_ref[...] = own[:own_rows].astype(jnp.bfloat16)
    nope = lax.dot_general(
        normed, query_ref[...], NT, preferred_element_type=jnp.float32
    ).astype(jnp.bfloat16)
    turned = lax.dot_general(normed, rotary_ref[...], NT, preferred_element_type=jnp.float32)
    projected = jnp.dot(nope, key_ref[...], preferred_element_type=jnp.float32)
    for t in range(peers):
        at = slice(t * own_rows, (t + 1) * own_rows)
        out_ref[t, :, :latent] = projected[at].astype(jnp.bfloat16)
        out_ref[t, :, latent:] = turned[at].astype(jnp.bfloat16)


def in_hbm(*arrays):
    return tuple(pltpu.with_memory_space_constraint(a, pltpu.HBM) for a in arrays)


def front(
    hidden, gain, query_weight, rotary_weight, key_up, ids, logits, lengths, peers, capacity,
):
    rows, features = hidden.shape
    own_rows = rows // peers
    rope, latent = rotary_weight.shape[1], key_up.shape[1]
    arrays = in_hbm(
        hidden, gain[None, :], query_weight.T, rotary_weight.T, key_up, ids.T, logits.T, lengths
    )
    held = [pltpu.VMEM(a.shape, a.dtype) for a in arrays[:-1]]
    return call(
        functools.partial(front_kernel, capacity),
        "front",
        (
            shape((peers, own_rows, latent + rope), jnp.bfloat16),
            shape((own_rows, features), jnp.bfloat16),
            shape((2, rows), jnp.float32),
            shape((rows, 4), jnp.float32),
            shape((3 * own_rows, rope), jnp.float32),
        ),
        [HBM] * 8,
        arrays,
        scratch=held + [pltpu.SMEM(lengths.shape, lengths.dtype), pltpu.SemaphoreType.DMA((8,))],
        flops=AHEAD,
    )


def attend_kernel(
    scale, query_ref, trig_ref, latent_ref, rope_ref, out_ref, latent_query, rotary_query, summed_ref
):
    rows, heads, width = latent_query.shape
    rope = rotary_query.shape[2]
    most = latent_ref.shape[1] // BLOCK
    lengths = [
        jnp.max(trig_ref[2 * rows + s : 2 * rows + s + 1, :]).astype(jnp.int32) for s in range(rows)
    ]
    counts = [lax.div(length + (BLOCK - 1), BLOCK) for length in lengths]

    swap = lax.broadcasted_iota(jnp.int32, (rope, rope), 0) == lax.rem(
        lax.broadcasted_iota(jnp.int32, (rope, rope), 1) + rope // 2, rope
    )
    swap = jnp.where(swap, 1.0, 0.0).astype(jnp.bfloat16)
    received = query_ref[...].astype(jnp.float32)
    query = jnp.concatenate(
        [received[h, s : s + 1, :] for s in range(rows) for h in range(heads)], axis=0
    )
    plain = query[:, width:]
    turned = jnp.dot(plain.astype(jnp.bfloat16), swap, preferred_element_type=jnp.float32)
    for s in range(rows):
        at = slice(s * heads, (s + 1) * heads)
        latent_query[s] = query[at, :width].astype(jnp.bfloat16)
        rotary_query[s] = (
            plain[at] * trig_ref[2 * s : 2 * s + 1, :]
            + turned[at] * trig_ref[2 * s + 1 : 2 * s + 2, :]
        ).astype(jnp.bfloat16)

    larger = jnp.where(counts[0] >= counts[1], 0, 1)
    order = (larger, 1 - larger)
    ordered = [jnp.where(s == 0, lengths[0], lengths[1]) for s in order]
    large, small = [lax.div(length + (BLOCK - 1), BLOCK) for length in ordered]

    def score(s, length, b, last):
        at = slice(b * BLOCK, (b + 1) * BLOCK)
        part = product(latent_query[s], latent_ref[s, at, :])
        part = part + jnp.dot(
            rotary_query[s], rope_ref[s, :, at], preferred_element_type=jnp.float32
        )
        part = part * scale
        if last:
            places = b * BLOCK + lax.broadcasted_iota(jnp.int32, (heads, BLOCK), 1)
            part = jnp.where(places < length, part, NEG)
        return part

    def soften(scores):
        highest = functools.reduce(jnp.maximum, scores)
        highest = jnp.max(highest, axis=1, keepdims=True)
        weights = [jnp.exp(part - highest) for part in scores]
        total = functools.reduce(jnp.add, weights)
        factor = 1.0 / jnp.sum(total, axis=1, keepdims=True)
        return [(part * factor).astype(jnp.bfloat16) for part in weights]

    def weigh(s, probs):
        terms = [
            jnp.dot(
                part, latent_ref[s, b * BLOCK : (b + 1) * BLOCK, :],
                preferred_element_type=jnp.float32,
            )
            for b, part in enumerate(probs)
        ]
        summed_ref[s] = functools.reduce(jnp.add, terms)

    for most_blocks in range(1, most + 1):
        for least_blocks in range(1, most_blocks + 1):

            @pl.when((large == most_blocks) & (small == least_blocks))
            def _attend(filled=(most_blocks, least_blocks)):
                scores = [
                    [score(s, length, b, b == count - 1) for b in range(count)]
                    for s, length, count in zip(order, ordered, filled)
                ]
                for s, parts in zip(order, scores):
                    weigh(s, soften(parts))

    sums = [summed_ref[s] for s in range(rows)]
    for h in range(heads):
        out_ref[h] = jnp.concatenate([part[h : h + 1, :] for part in sums], axis=0).astype(
            jnp.bfloat16
        )


def attend(query, trig, latent, rotary, scale):
    rows, most, width = latent.shape
    heads, rope = query.shape[0], rotary.shape[1]
    return call(
        functools.partial(attend_kernel, scale),
        "attend",
        shape((heads, rows, width), jnp.bfloat16),
        [VMEM] * 4,
        (query, trig, latent, rotary),
        scratch=(
            pltpu.VMEM((rows, heads, width), jnp.bfloat16),
            pltpu.VMEM((rows, heads, rope), jnp.bfloat16),
            pltpu.VMEM((rows, heads, width), jnp.float32),
        ),
        limit=ATTEND_LIMIT,
        flops=4 * latent.size * heads,
    )


def row_sums(terms, rows, keep):
    place = lax.broadcasted_iota(jnp.int32, (8, terms.shape[0]), 1)
    wanted = (lax.rem(place, rows) == lax.broadcasted_iota(jnp.int32, place.shape, 0)) & keep(place)
    ones = jnp.where(wanted, 1.0, 0.0).astype(jnp.bfloat16)
    return jnp.dot(ones, terms, preferred_element_type=jnp.float32)


def mix_kernel(terms_ref, own_ref, mixed_gain_ref, moe_gain_ref, mixed_ref, send_ref):
    peers, rows, half = send_ref.shape
    attended = row_sums(terms_ref[...], rows, lambda place: place >= 0)[:rows].astype(jnp.bfloat16)
    mixed = (
        own_ref[...].astype(jnp.float32) + norm_rows(attended, mixed_gain_ref[...])
    ).astype(jnp.bfloat16)
    mixed_ref[...] = mixed
    normed = norm_rows(mixed, moe_gain_ref[...]).astype(jnp.bfloat16)
    for t in range(peers):
        send_ref[t] = normed[:, (t % 2) * half : (t % 2 + 1) * half]


def mix(terms, own, mixed_gain, moe_gain, peers):
    rows, features = own.shape
    return call(
        mix_kernel,
        "mix",
        (
            shape((rows, features), jnp.bfloat16),
            shape((peers, rows, features // 2), jnp.bfloat16),
        ),
        [VMEM] * 4,
        (terms, own, mixed_gain[None, :], moe_gain[None, :]),
    )


def dispatch_kernel(slots_ref, rows_ref, out_ref):
    slots, rows = out_ref.shape[0], rows_ref.shape[0]
    place = lax.broadcasted_iota(jnp.int32, (slots, rows), 0).astype(jnp.float32)
    taken = (place == slots_ref[0:1, :]) | (place == slots_ref[1:2, :])
    pick = jnp.where(taken, 1.0, 0.0).astype(jnp.bfloat16)
    out_ref[...] = jnp.dot(pick, rows_ref[...], preferred_element_type=jnp.float32).astype(
        jnp.bfloat16
    )


def dispatch(own_slots, rows, slots):
    return call(
        dispatch_kernel,
        "dispatch",
        shape((slots, rows.shape[1]), jnp.bfloat16),
        [VMEM] * 2,
        (own_slots, rows),
        flops=AHEAD,
    )


def combine_kernel(columns_ref, returned_ref, out_ref):
    rows, slots = out_ref.shape[0], returned_ref.shape[0]
    place = lax.broadcasted_iota(jnp.int32, (rows, slots), 1).astype(jnp.float32)
    gates = jnp.where(place == columns_ref[:, 0:1], columns_ref[:, 2:3], 0.0)
    gates = gates + jnp.where(place == columns_ref[:, 1:2], columns_ref[:, 3:4], 0.0)
    returned = returned_ref[...]
    parts = []
    for _ in range(3):
        parts.append(gates.astype(jnp.bfloat16))
        gates = gates - parts[-1].astype(jnp.float32)
    terms = jnp.dot(
        jnp.concatenate(parts, axis=0), returned, preferred_element_type=jnp.float32
    )
    total = terms[:rows] + terms[rows : 2 * rows] + terms[2 * rows :]
    out_ref[...] = total.astype(jnp.bfloat16)


def combine(columns, returned):
    return call(
        combine_kernel,
        "combine",
        shape((columns.shape[0], returned.shape[1]), jnp.bfloat16),
        [VMEM] * 2,
        (columns, returned),
    )


def finish_kernel(terms_ref, mixed_ref, gain_ref, out_ref):
    rows = mixed_ref.shape[0]
    terms = terms_ref[...]
    halves = [
        row_sums(terms, rows, lambda place, c=c: lax.rem(lax.div(place, rows), 2) == c)
        for c in range(2)
    ]
    routed = jnp.concatenate(halves, axis=1)[:rows].astype(jnp.bfloat16)
    out_ref[...] = (
        mixed_ref[...].astype(jnp.float32) + norm_rows(routed, gain_ref[...])
    ).astype(jnp.bfloat16)


def finish(terms, mixed, gain):
    return call(
        finish_kernel,
        "finish",
        shape(mixed.shape, jnp.bfloat16),
        [VMEM] * 3,
        (terms, mixed, gain[None, :]),
    )


def half_at(own, half):
    core = lax.rem(lax.axis_index("tp"), 2)
    if not own:
        core = 1 - core
    return pl.ds(pl.multiple_of(core * half, half), half)


def product(rows, weight):
    return lax.dot_general(rows, weight, NT, preferred_element_type=jnp.float32)


def enter_kernel(rows_ref, gate_ref, up_ref, down_ref, gate_out, up_out):
    del down_ref
    rows = rows_ref[...]
    at = half_at(True, rows.shape[1])
    gate_out[...] = product(rows, gate_ref[:, at])
    up_out[...] = product(rows, up_ref[:, at])


def leave_kernel(rows_ref, gate_ref, up_ref, down_ref, gate_part, up_part, act_ref, out_ref):
    rows = rows_ref[...]
    at = half_at(False, rows.shape[1])
    gate = gate_part[...] + product(rows, gate_ref[:, at])
    up = up_part[...] + product(rows, up_ref[:, at])
    act = (gate / (1.0 + jnp.exp(-gate)) * up).astype(jnp.bfloat16)
    act_ref[...] = act
    out_ref[...] = jnp.dot(act, down_ref[:, at], preferred_element_type=jnp.float32).astype(
        jnp.bfloat16
    )


def close_kernel(act_ref, down_ref, out_ref):
    at = half_at(True, out_ref.shape[1])
    out_ref[...] = jnp.dot(act_ref[...], down_ref[:, at], preferred_element_type=jnp.float32)


def expert_rows(rows, gate_weight, up_weight, down_weight, pairs):
    slots, half = rows.shape
    width = gate_weight.shape[0]
    part = shape((slots, width), jnp.float32)
    other = lax.ppermute(rows, "tp", pairs)
    gate_part, up_part = call(
        enter_kernel,
        "enter",
        (part, part),
        [VMEM] * 4,
        (rows, gate_weight, up_weight, down_weight),
        flops=4 * slots * half * width,
    )
    act, sent = call(
        leave_kernel,
        "leave",
        (shape((slots, width), jnp.bfloat16), shape((slots, half), jnp.bfloat16)),
        [VMEM] * 6,
        (other, gate_weight, up_weight, down_weight, gate_part, up_part),
        flops=6 * slots * half * width,
    )
    arrived = lax.ppermute(sent, "tp", pairs)
    kept = call(
        close_kernel,
        "close",
        shape((slots, half), jnp.float32),
        [VMEM] * 2,
        (act, down_weight),
        flops=2 * slots * half * width,
    )
    return (kept + arrived.astype(jnp.float32)).astype(jnp.bfloat16)


def exchanged(array, axis):
    return lax.all_to_all(array, axis, split_axis=0, concat_axis=0, tiled=True)


def body(
    hidden,
    attn_gain,
    query_weight,
    rotary_weight,
    key_up,
    cache_latent,
    cache_rotary,
    lengths,
    value_up,
    out_weight,
    mixed_gain,
    moe_gain,
    expert_ids,
    route_logits,
    gate_weight,
    up_weight,
    down_weight,
    final_gain,
):
    group_rows, features = hidden.shape
    _, nope_width, latent_width = key_up.shape
    rotary_width = rotary_weight.shape[1]
    own_rows = cache_latent.shape[0]
    groups = lax.axis_size("ep")
    peers = lax.axis_size("tp")
    pairs = [(i, i ^ 1) for i in range(peers)]
    half = features // 2
    capacity = 2 * group_rows * expert_ids.shape[1] // groups
    slots = groups * capacity

    query, own_hidden, own_slots, columns, trig = front(
        hidden,
        attn_gain,
        query_weight,
        rotary_weight,
        key_up[0],
        expert_ids,
        route_logits,
        lengths,
        peers,
        capacity,
    )
    query = exchanged(query, "tp")
    score_scale = (nope_width + rotary_width) ** (-0.5)
    out_latent = attend(
        query, trig, cache_latent, cache_rotary, score_scale
    )
    out_latent = exchanged(out_latent, "tp")
    out_latent = out_latent.reshape(group_rows, latent_width)
    head_out = jnp.dot(out_latent, value_up[0], preferred_element_type=jnp.float32)
    head_terms = jnp.dot(
        head_out.astype(jnp.bfloat16), out_weight, preferred_element_type=jnp.float32
    )
    head_terms = head_terms.astype(jnp.bfloat16).reshape(peers, own_rows, features)
    head_terms = exchanged(head_terms, "tp").reshape(group_rows, features)
    mixed_rows, normed = mix(head_terms, own_hidden, mixed_gain, moe_gain, peers)
    normed = exchanged(normed, "tp").reshape(group_rows, half)
    outgoing = dispatch(own_slots, normed, slots).reshape(groups, capacity, half)
    arrived = exchanged(outgoing, "ep").reshape(slots, half)
    result = expert_rows(arrived, gate_weight[0].T, up_weight[0].T, down_weight[0], pairs)
    returned = exchanged(result.reshape(groups, capacity, half), "ep").reshape(slots, half)
    combined = combine(columns, returned).reshape(peers, own_rows, half)
    terms = exchanged(combined, "tp").reshape(group_rows, half)
    return finish(terms, mixed_rows, final_gain)


def solution(mesh):
    placed = (
        P("ep", None),
        P(),
        P(None, "tp"),
        P(None, "tp"),
        P("tp", None, None),
        P(("ep", "tp"), None, None),
        P(("ep", "tp"), None, None),
        P(("ep", "tp")),
        P("tp", None, None),
        P("tp", None),
        P(),
        P(),
        P(),
        P(),
        P("ep", None, "tp"),
        P("ep", None, "tp"),
        P("ep", "tp", None),
        P(),
    )
    return jax.shard_map(
        body, mesh=mesh, in_specs=placed, out_specs=P(("ep", "tp"), None), check_vma=False
    )
```

```python
import functools

import jax
import jax.numpy as jnp
import numpy as np
from jax import lax
from jax.experimental import pallas as pl
from jax.experimental.pallas import tpu as pltpu
from jax.sharding import PartitionSpec as P

EPSILON = 1e-06
BLOCK = 1024
NEG = float("-inf")
VMEM = pl.BlockSpec(memory_space=pltpu.VMEM)
SMEM = pl.BlockSpec(memory_space=pltpu.SMEM)
HBM = pl.BlockSpec(memory_space=pltpu.HBM)
AHEAD = 10**10
ATTEND_LIMIT = 2 * 1024 * 1024
SMALL_LIMIT = 4 * 1024 * 1024
NT = (((1,), (1,)), ((), ()))


def call(kernel, name, outs, ins, args, scratch=(), limit=SMALL_LIMIT, flops=0):
    return pl.pallas_call(
        kernel,
        out_shape=outs,
        in_specs=ins,
        out_specs=jax.tree.map(lambda _: VMEM, outs),
        scratch_shapes=list(scratch),
        compiler_params=pltpu.CompilerParams(vmem_limit_bytes=limit),
        cost_estimate=pl.CostEstimate(flops=flops, bytes_accessed=0, transcendentals=0),
        name=name,
    )(*args)


def shape(dims, dtype):
    return jax.ShapeDtypeStruct(dims, dtype)


def norm_rows(values, gain_vector):
    values = values.astype(jnp.float32)
    factor = lax.rsqrt(jnp.mean(values * values, axis=-1, keepdims=True) + EPSILON)
    return values * factor * gain_vector


def column(row):
    size = row.shape[1]
    same = lax.broadcasted_iota(jnp.int32, (size, size), 0) == lax.broadcasted_iota(
        jnp.int32, (size, size), 1
    )
    return jnp.sum(jnp.where(same, row, 0.0), axis=1, keepdims=True)


def front_kernel(
    capacity, hidden_hbm, gain_hbm, query_hbm, rotary_hbm, key_hbm, ids_hbm, logits_hbm, lengths_hbm,
    out_ref, own_ref, slots_ref, columns_ref, trig_ref,
    hidden_ref, gain_ref, query_ref, rotary_ref, key_ref, ids_ref, logits_ref, lengths_ref, sems,
):
    group_rows, features = hidden_ref.shape
    peers, own_rows, _ = out_ref.shape
    latent = key_ref.shape[1]
    pairs = (
        (lengths_hbm, lengths_ref),
        (ids_hbm, ids_ref),
        (logits_hbm, logits_ref),
        (hidden_hbm, hidden_ref),
        (gain_hbm, gain_ref),
        (query_hbm, query_ref),
        (rotary_hbm, rotary_ref),
        (key_hbm, key_ref),
    )
    copies = [pltpu.make_async_copy(s, d, sems.at[i]) for i, (s, d) in enumerate(pairs)]
    for copy in copies:
        copy.start()
    group, place = lax.axis_index("ep"), lax.axis_index("tp")
    for copy in copies:
        copy.wait()
    ids_all = ids_ref[...].astype(jnp.float32)
    logits_all = logits_ref[...]
    ids = jnp.zeros((2, group_rows), jnp.float32)
    logits = jnp.zeros((2, group_rows), jnp.float32)
    for g in range(ids_all.shape[1] // group_rows):
        at = slice(g * group_rows, (g + 1) * group_rows)
        ids = jnp.where(group == g, ids_all[:, at], ids)
        logits = jnp.where(group == g, logits_all[:, at], logits)
    id_rows = [ids[k : k + 1, :] for k in range(2)]
    id_columns = [column(row) for row in id_rows]
    before = lax.broadcasted_iota(jnp.int32, (group_rows, group_rows), 0) < lax.broadcasted_iota(
        jnp.int32, (group_rows, group_rows), 1
    )
    top = jnp.maximum(logits[0:1, :], logits[1:2, :])
    weights = [jnp.exp(logits[k : k + 1, :] - top) for k in range(2)]
    for k in range(2):
        hits = jnp.where(before & (id_columns[0] == id_rows[k]), 1.0, 0.0)
        hits = hits + jnp.where(before & (id_columns[1] == id_rows[k]), 1.0, 0.0)
        slot = id_rows[k] * capacity + jnp.sum(hits, axis=0, keepdims=True)
        slots_ref[k : k + 1, :] = slot
        columns_ref[:, k : k + 1] = column(slot)
        columns_ref[:, 2 + k : 3 + k] = column(weights[k] / (weights[0] + weights[1]))

    half = trig_ref.shape[1] // 2
    lane = lax.broadcasted_iota(jnp.int32, (1, 2 * half), 1)
    inverse = jnp.zeros((1, 2 * half), jnp.float32)
    for i in range(half):
        value = float(np.float32(10000.0 ** (-i / half)))
        inverse = jnp.where((lane == i) | (lane == i + half), value, inverse)
    for s in range(own_rows):
        angles = (lengths_ref[s] - 1).astype(jnp.float32) * inverse
        turned = jnp.sin(angles)
        trig_ref[2 * s : 2 * s + 1, :] = jnp.cos(angles)
        trig_ref[2 * s + 1 : 2 * s + 2, :] = jnp.where(lane < half, -turned, turned)
        at = 2 * own_rows + s
        trig_ref[at : at + 1, :] = jnp.zeros_like(angles) + lengths_ref[s].astype(jnp.float32)

    hidden = hidden_ref[...]
    normed = norm_rows(hidden, gain_ref[...]).astype(jnp.bfloat16)
    pick_row = lax.broadcasted_iota(jnp.int32, (8, group_rows), 0) + place * own_rows
    pick = jnp.where(pick_row == lax.broadcasted_iota(jnp.int32, (8, group_rows), 1), 1.0, 0.0)
    own = jnp.dot(pick.astype(jnp.bfloat16), hidden, preferred_element_type=jnp.float32)
    own_ref[...] = own[:own_rows].astype(jnp.bfloat16)
    nope = lax.dot_general(
        normed, query_ref[...], NT, preferred_element_type=jnp.float32
    ).astype(jnp.bfloat16)
    turned = lax.dot_general(normed, rotary_ref[...], NT, preferred_element_type=jnp.float32)
    projected = jnp.dot(nope, key_ref[...], preferred_element_type=jnp.float32)
    for t in range(peers):
        at = slice(t * own_rows, (t + 1) * own_rows)
        out_ref[t, :, :latent] = projected[at].astype(jnp.bfloat16)
        out_ref[t, :, latent:] = turned[at].astype(jnp.bfloat16)


def in_hbm(*arrays):
    return tuple(pltpu.with_memory_space_constraint(a, pltpu.HBM) for a in arrays)


def front(
    hidden, gain, query_weight, rotary_weight, key_up, ids, logits, lengths, peers, capacity,
):
    rows, features = hidden.shape
    own_rows = rows // peers
    rope, latent = rotary_weight.shape[1], key_up.shape[1]
    arrays = in_hbm(
        hidden, gain[None, :], query_weight.T, rotary_weight.T, key_up, ids.T, logits.T, lengths
    )
    held = [pltpu.VMEM(a.shape, a.dtype) for a in arrays[:-1]]
    return call(
        functools.partial(front_kernel, capacity),
        "front",
        (
            shape((peers, own_rows, latent + rope), jnp.bfloat16),
            shape((own_rows, features), jnp.bfloat16),
            shape((2, rows), jnp.float32),
            shape((rows, 4), jnp.float32),
            shape((3 * own_rows, rope), jnp.float32),
        ),
        [HBM] * 8,
        arrays,
        scratch=held + [pltpu.SMEM(lengths.shape, lengths.dtype), pltpu.SemaphoreType.DMA((8,))],
        flops=AHEAD,
    )


def attend_kernel(
    scale, query_ref, trig_ref, latent_ref, rope_ref, out_ref, latent_query, rotary_query, summed_ref
):
    rows, heads, width = latent_query.shape
    rope = rotary_query.shape[2]
    most = latent_ref.shape[1] // BLOCK
    lengths = [
        jnp.max(trig_ref[2 * rows + s : 2 * rows + s + 1, :]).astype(jnp.int32) for s in range(rows)
    ]
    counts = [lax.div(length + (BLOCK - 1), BLOCK) for length in lengths]

    swap = lax.broadcasted_iota(jnp.int32, (rope, rope), 0) == lax.rem(
        lax.broadcasted_iota(jnp.int32, (rope, rope), 1) + rope // 2, rope
    )
    swap = jnp.where(swap, 1.0, 0.0).astype(jnp.bfloat16)
    received = query_ref[...].astype(jnp.float32)
    query = jnp.concatenate(
        [received[h, s : s + 1, :] for s in range(rows) for h in range(heads)], axis=0
    )
    plain = query[:, width:]
    turned = jnp.dot(plain.astype(jnp.bfloat16), swap, preferred_element_type=jnp.float32)
    for s in range(rows):
        at = slice(s * heads, (s + 1) * heads)
        latent_query[s] = query[at, :width].astype(jnp.bfloat16)
        rotary_query[s] = (
            plain[at] * trig_ref[2 * s : 2 * s + 1, :]
            + turned[at] * trig_ref[2 * s + 1 : 2 * s + 2, :]
        ).astype(jnp.bfloat16)

    larger = jnp.where(counts[0] >= counts[1], 0, 1)
    order = (larger, 1 - larger)
    ordered = [jnp.where(s == 0, lengths[0], lengths[1]) for s in order]
    large, small = [lax.div(length + (BLOCK - 1), BLOCK) for length in ordered]

    def score(s, length, b, last):
        at = slice(b * BLOCK, (b + 1) * BLOCK)
        part = product(latent_query[s], latent_ref[s, at, :])
        part = part + jnp.dot(
            rotary_query[s], rope_ref[s, :, at], preferred_element_type=jnp.float32
        )
        part = part * scale
        if last:
            places = b * BLOCK + lax.broadcasted_iota(jnp.int32, (heads, BLOCK), 1)
            part = jnp.where(places < length, part, NEG)
        return part

    def soften(scores):
        highest = functools.reduce(jnp.maximum, scores)
        highest = jnp.max(highest, axis=1, keepdims=True)
        weights = [jnp.exp(part - highest) for part in scores]
        total = functools.reduce(jnp.add, weights)
        factor = 1.0 / jnp.sum(total, axis=1, keepdims=True)
        return [(part * factor).astype(jnp.bfloat16) for part in weights]

    def weigh(s, probs):
        terms = [
            jnp.dot(
                part, latent_ref[s, b * BLOCK : (b + 1) * BLOCK, :],
                preferred_element_type=jnp.float32,
            )
            for b, part in enumerate(probs)
        ]
        summed_ref[s] = functools.reduce(jnp.add, terms)

    for most_blocks in range(1, most + 1):
        for least_blocks in range(1, most_blocks + 1):

            @pl.when((large == most_blocks) & (small == least_blocks))
            def _attend(filled=(most_blocks, least_blocks)):
                scores = [
                    [score(s, length, b, b == count - 1) for b in range(count)]
                    for s, length, count in zip(order, ordered, filled)
                ]
                for s, parts in zip(order, scores):
                    weigh(s, soften(parts))

    sums = [summed_ref[s] for s in range(rows)]
    for h in range(heads):
        out_ref[h] = jnp.concatenate([part[h : h + 1, :] for part in sums], axis=0).astype(
            jnp.bfloat16
        )


def attend(query, trig, latent, rotary, scale):
    rows, most, width = latent.shape
    heads, rope = query.shape[0], rotary.shape[1]
    return call(
        functools.partial(attend_kernel, scale),
        "attend",
        shape((heads, rows, width), jnp.bfloat16),
        [VMEM] * 4,
        (query, trig, latent, rotary),
        scratch=(
            pltpu.VMEM((rows, heads, width), jnp.bfloat16),
            pltpu.VMEM((rows, heads, rope), jnp.bfloat16),
            pltpu.VMEM((rows, heads, width), jnp.float32),
        ),
        limit=ATTEND_LIMIT,
        flops=4 * latent.size * heads,
    )


def heads_kernel(latent_ref, value_ref, out_weight_ref, terms_ref):
    peers, rows, _ = terms_ref.shape
    head_out = product(latent_ref[...], value_ref[...]).astype(jnp.bfloat16)
    terms = jnp.dot(head_out, out_weight_ref[...], preferred_element_type=jnp.float32)
    for t in range(peers):
        terms_ref[t] = terms[t * rows : (t + 1) * rows].astype(jnp.bfloat16)


def heads_terms(latents, value, out_weight, peers):
    return call(
        heads_kernel,
        "heads",
        shape((peers, latents.shape[0] // peers, out_weight.shape[1]), jnp.bfloat16),
        [VMEM] * 3,
        (latents, value, out_weight),
    )


def row_sums(terms, rows, keep):
    place = lax.broadcasted_iota(jnp.int32, (8, terms.shape[0]), 1)
    wanted = (lax.rem(place, rows) == lax.broadcasted_iota(jnp.int32, place.shape, 0)) & keep(place)
    ones = jnp.where(wanted, 1.0, 0.0).astype(jnp.bfloat16)
    return jnp.dot(ones, terms, preferred_element_type=jnp.float32)


def mix_kernel(terms_ref, own_ref, mixed_gain_ref, moe_gain_ref, mixed_ref, send_ref):
    peers, rows, half = send_ref.shape
    attended = row_sums(terms_ref[...], rows, lambda place: place >= 0)[:rows].astype(jnp.bfloat16)
    mixed = (
        own_ref[...].astype(jnp.float32) + norm_rows(attended, mixed_gain_ref[...])
    ).astype(jnp.bfloat16)
    mixed_ref[...] = mixed
    normed = norm_rows(mixed, moe_gain_ref[...]).astype(jnp.bfloat16)
    for t in range(peers):
        send_ref[t] = normed[:, (t % 2) * half : (t % 2 + 1) * half]


def mix(terms, own, mixed_gain, moe_gain, peers):
    rows, features = own.shape
    return call(
        mix_kernel,
        "mix",
        (
            shape((rows, features), jnp.bfloat16),
            shape((peers, rows, features // 2), jnp.bfloat16),
        ),
        [VMEM] * 4,
        (terms, own, mixed_gain[None, :], moe_gain[None, :]),
    )


def dispatch_kernel(slots_ref, rows_ref, out_ref):
    slots, rows = out_ref.shape[0], rows_ref.shape[0]
    place = lax.broadcasted_iota(jnp.int32, (slots, rows), 0).astype(jnp.float32)
    taken = (place == slots_ref[0:1, :]) | (place == slots_ref[1:2, :])
    pick = jnp.where(taken, 1.0, 0.0).astype(jnp.bfloat16)
    out_ref[...] = jnp.dot(pick, rows_ref[...], preferred_element_type=jnp.float32).astype(
        jnp.bfloat16
    )


def dispatch(own_slots, rows, slots):
    return call(
        dispatch_kernel,
        "dispatch",
        shape((slots, rows.shape[1]), jnp.bfloat16),
        [VMEM] * 2,
        (own_slots, rows),
        flops=AHEAD,
    )


def combine_kernel(columns_ref, returned_ref, out_ref):
    rows, slots = out_ref.shape[0], returned_ref.shape[0]
    place = lax.broadcasted_iota(jnp.int32, (rows, slots), 1).astype(jnp.float32)
    gates = jnp.where(place == columns_ref[:, 0:1], columns_ref[:, 2:3], 0.0)
    gates = gates + jnp.where(place == columns_ref[:, 1:2], columns_ref[:, 3:4], 0.0)
    returned = returned_ref[...]
    parts = []
    for _ in range(3):
        parts.append(gates.astype(jnp.bfloat16))
        gates = gates - parts[-1].astype(jnp.float32)
    terms = jnp.dot(
        jnp.concatenate(parts, axis=0), returned, preferred_element_type=jnp.float32
    )
    total = terms[:rows] + terms[rows : 2 * rows] + terms[2 * rows :]
    out_ref[...] = total.astype(jnp.bfloat16)


def combine(columns, returned):
    return call(
        combine_kernel,
        "combine",
        shape((columns.shape[0], returned.shape[1]), jnp.bfloat16),
        [VMEM] * 2,
        (columns, returned),
    )


def finish_kernel(terms_ref, mixed_ref, gain_ref, out_ref):
    rows = mixed_ref.shape[0]
    terms = terms_ref[...]
    halves = [
        row_sums(terms, rows, lambda place, c=c: lax.rem(lax.div(place, rows), 2) == c)
        for c in range(2)
    ]
    routed = jnp.concatenate(halves, axis=1)[:rows].astype(jnp.bfloat16)
    out_ref[...] = (
        mixed_ref[...].astype(jnp.float32) + norm_rows(routed, gain_ref[...])
    ).astype(jnp.bfloat16)


def finish(terms, mixed, gain):
    return call(
        finish_kernel,
        "finish",
        shape(mixed.shape, jnp.bfloat16),
        [VMEM] * 3,
        (terms, mixed, gain[None, :]),
    )


def half_at(own, half):
    core = lax.rem(lax.axis_index("tp"), 2)
    if not own:
        core = 1 - core
    return pl.ds(pl.multiple_of(core * half, half), half)


def product(rows, weight):
    return lax.dot_general(rows, weight, NT, preferred_element_type=jnp.float32)


def enter_kernel(rows_ref, gate_ref, up_ref, down_ref, gate_out, up_out):
    del down_ref
    rows = rows_ref[...]
    at = half_at(True, rows.shape[1])
    gate_out[...] = product(rows, gate_ref[:, at])
    up_out[...] = product(rows, up_ref[:, at])


def leave_kernel(rows_ref, gate_ref, up_ref, down_ref, gate_part, up_part, act_ref, out_ref):
    rows = rows_ref[...]
    at = half_at(False, rows.shape[1])
    gate = gate_part[...] + product(rows, gate_ref[:, at])
    up = up_part[...] + product(rows, up_ref[:, at])
    act = (gate / (1.0 + jnp.exp(-gate)) * up).astype(jnp.bfloat16)
    act_ref[...] = act
    out_ref[...] = jnp.dot(act, down_ref[:, at], preferred_element_type=jnp.float32).astype(
        jnp.bfloat16
    )


def close_kernel(act_ref, down_ref, out_ref):
    at = half_at(True, out_ref.shape[1])
    out_ref[...] = jnp.dot(act_ref[...], down_ref[:, at], preferred_element_type=jnp.float32)


def expert_rows(rows, gate_weight, up_weight, down_weight, pairs):
    slots, half = rows.shape
    width = gate_weight.shape[0]
    part = shape((slots, width), jnp.float32)
    other = lax.ppermute(rows, "tp", pairs)
    gate_part, up_part = call(
        enter_kernel,
        "enter",
        (part, part),
        [VMEM] * 4,
        (rows, gate_weight, up_weight, down_weight),
        flops=4 * slots * half * width,
    )
    act, sent = call(
        leave_kernel,
        "leave",
        (shape((slots, width), jnp.bfloat16), shape((slots, half), jnp.bfloat16)),
        [VMEM] * 6,
        (other, gate_weight, up_weight, down_weight, gate_part, up_part),
        flops=6 * slots * half * width,
    )
    arrived = lax.ppermute(sent, "tp", pairs)
    kept = call(
        close_kernel,
        "close",
        shape((slots, half), jnp.float32),
        [VMEM] * 2,
        (act, down_weight),
        flops=2 * slots * half * width,
    )
    return (kept + arrived.astype(jnp.float32)).astype(jnp.bfloat16)


def exchanged(array, axis):
    return lax.all_to_all(array, axis, split_axis=0, concat_axis=0, tiled=True)


def body(
    hidden,
    attn_gain,
    query_weight,
    rotary_weight,
    key_up,
    cache_latent,
    cache_rotary,
    lengths,
    value_up,
    out_weight,
    mixed_gain,
    moe_gain,
    expert_ids,
    route_logits,
    gate_weight,
    up_weight,
    down_weight,
    final_gain,
):
    group_rows, features = hidden.shape
    _, nope_width, latent_width = key_up.shape
    rotary_width = rotary_weight.shape[1]
    own_rows = cache_latent.shape[0]
    groups = lax.axis_size("ep")
    peers = lax.axis_size("tp")
    pairs = [(i, i ^ 1) for i in range(peers)]
    half = features // 2
    capacity = 2 * group_rows * expert_ids.shape[1] // groups
    slots = groups * capacity

    query, own_hidden, own_slots, columns, trig = front(
        hidden,
        attn_gain,
        query_weight,
        rotary_weight,
        key_up[0],
        expert_ids,
        route_logits,
        lengths,
        peers,
        capacity,
    )
    query = exchanged(query, "tp")
    score_scale = (nope_width + rotary_width) ** (-0.5)
    out_latent = attend(
        query, trig, cache_latent, cache_rotary, score_scale
    )
    out_latent = exchanged(out_latent, "tp")
    out_latent = out_latent.reshape(group_rows, latent_width)
    head_terms = heads_terms(out_latent, value_up[0].T, out_weight, peers)
    head_terms = exchanged(head_terms, "tp").reshape(group_rows, features)
    mixed_rows, normed = mix(head_terms, own_hidden, mixed_gain, moe_gain, peers)
    normed = exchanged(normed, "tp").reshape(group_rows, half)
    outgoing = dispatch(own_slots, normed, slots).reshape(groups, capacity, half)
    arrived = exchanged(outgoing, "ep").reshape(slots, half)
    result = expert_rows(arrived, gate_weight[0].T, up_weight[0].T, down_weight[0], pairs)
    returned = exchanged(result.reshape(groups, capacity, half), "ep").reshape(slots, half)
    combined = combine(columns, returned).reshape(peers, own_rows, half)
    terms = exchanged(combined, "tp").reshape(group_rows, half)
    return finish(terms, mixed_rows, final_gain)


def solution(mesh):
    placed = (
        P("ep", None),
        P(),
        P(None, "tp"),
        P(None, "tp"),
        P("tp", None, None),
        P(("ep", "tp"), None, None),
        P(("ep", "tp"), None, None),
        P(("ep", "tp")),
        P("tp", None, None),
        P("tp", None),
        P(),
        P(),
        P(),
        P(),
        P("ep", None, "tp"),
        P("ep", None, "tp"),
        P("ep", "tp", None),
        P(),
    )
    return jax.shard_map(
        body, mesh=mesh, in_specs=placed, out_specs=P(("ep", "tp"), None), check_vma=False
    )
```
